128 devices in a mesh: ep: 16 (over z, x), tp: 8 (over y, core).
Axes of the slice: x: 4, y: 4, z: 4, core: 2. Of those that a mesh axis runs over, the one named last changes fastest.
Arguments:
- tokens: bfloat16 [16384, 2048], P(('ep', 'tp')), may hold values from -6 to 6
- routes: int32 [16384, 2], P(('ep', 'tp')), may hold values from 0 to 127, as said below
- gates: float32 [16384, 2], P(('ep', 'tp')), may hold values from 0.1 to 0.6
- w_gate: bfloat16 [128, 2048, 768], P(('ep', 'tp')), may hold values from -0.125 to 0.125
- w_up: bfloat16 [128, 2048, 768], P(('ep', 'tp')), may hold values from -0.125 to 0.125
- w_down: bfloat16 [128, 768, 2048], P(('ep', 'tp')), may hold values from -0.21875 to 0.21875
- moe_out: bfloat16 [16384, 2048], P('ep', 'tp'), may hold values from -16 to 16
- norm_gain: float32 [2048], P('tp'), may hold values from 0.1 to 1.9
- out_grad: bfloat16 [16384, 2048], P('ep', 'tp'), may hold values from -16 to 16
Outputs:
- token_grad: bfloat16 [16384, 2048], P(('ep', 'tp'))
- gates_grad: bfloat16 [16384, 2], P(('ep', 'tp'))
- w_gate_grad: bfloat16 [128, 2048, 768], P(('ep', 'tp'))
- w_up_grad: bfloat16 [128, 2048, 768], P(('ep', 'tp'))
- w_down_grad: bfloat16 [128, 768, 2048], P(('ep', 'tp'))
The draws below stay inside these ranges and needn't reach their ends.
Inputs may be any that keep to these rules, and one draw needn't show every extreme that they name: `routes`: the two experts of a row differ and lie in one group (expert e is in group e // 32). In the 128 rows of one device the tokens fall into the groups in shares 3/8, 3/8, 1/8, 1/8 of 128, which group takes which share varying. In the rows of one device no expert is named more than 4 times, and one expert is named exactly 4 times in the rows of every device.
All inputs are finite; a program needn't handle non-finite values.
Results may differ from the reference program's by a relative error of at most 0.0071.
Values may be sent and summed in bfloat16 or wider, within the bound.
A program may use at most 128 MiB of HBM per device.

```python
import jax
import jax.numpy as jnp
from jax import lax

D = 2048
F = 768
GROUPS = 4
TOPK = 2
TOK_DEV = 128
EXPERTS = 128
EXP_GROUP = 32
CAP = 4
TOKENS = 16384


def draw_routes(key, part):
    tickets = EXP_GROUP * CAP
    shares = [3 * TOK_DEV // 8, 3 * TOK_DEV // 8, TOK_DEV // 8, TOK_DEV // 8]
    hot_global = jax.random.randint(jax.random.fold_in(key, 11), (), 0, EXPERTS)

    def one_block(block_key):
        sub_keys = jax.random.split(block_key, 4)
        group_order = jax.random.permutation(sub_keys[0], GROUPS)
        token_order = jax.random.permutation(sub_keys[1], TOK_DEV)
        hot_inner = jax.random.randint(sub_keys[2], (GROUPS,), 0, EXP_GROUP)
        noise_draw = jax.random.randint(sub_keys[3], (GROUPS, tickets), 0, 2 ** 19)
        ticket_ids = jnp.arange(tickets, dtype=jnp.int32)
        inner_ids = ticket_ids // CAP
        result = jnp.zeros((TOK_DEV, 2), jnp.int32)
        offset = 0
        for rank in range(GROUPS):
            expert_ids = group_order[rank] * EXP_GROUP + inner_ids
            hot_flag = jnp.logical_or(inner_ids == hot_inner[rank], expert_ids == hot_global).astype(jnp.int32)
            score_value = (hot_flag * 2 ** 19 + noise_draw[rank]) * tickets + ticket_ids
            share_size = shares[rank]
            picked = lax.top_k(score_value, 2 * share_size)[1]
            chosen = jnp.sort(expert_ids[picked])
            places = token_order[offset:offset + share_size]
            result = result.at[places, 0].set(chosen[:share_size])
            result = result.at[places, 1].set(chosen[share_size:])
            offset = offset + share_size
        return result
    block_keys = jax.random.split(jax.random.fold_in(key, 12), TOKENS // TOK_DEV)
    return jax.vmap(one_block)(block_keys).reshape(TOKENS, 2).astype(jnp.int32)


def paired_fields(key):
    sub_keys = jax.random.split(jax.random.fold_in(key, 21), 5)
    base = jax.random.normal(sub_keys[0], (TOKENS, D), jnp.float32)
    block_scale = jnp.exp(jax.random.uniform(sub_keys[1], (8,), jnp.float32, -1.2, 1.2))
    fine_scale = jnp.exp(jax.random.uniform(sub_keys[2], (D,), jnp.float32, -0.35, 0.35))
    columns = jnp.arange(D) * 8 // D
    col_scale = block_scale[columns] * fine_scale
    saved_out = jnp.clip(base * col_scale[None, :], -16.0, 16.0)
    noise_part = jax.random.normal(sub_keys[4], (TOKENS, D), jnp.float32)
    cotangent = jnp.clip(0.6 * base + 0.8 * noise_part, -16.0, 16.0)
    return (saved_out, cotangent)


def draw_moe_out(key, part):
    return paired_fields(key)[0].astype(jnp.bfloat16)


def draw_out_grad(key, part):
    return paired_fields(key)[1].astype(jnp.bfloat16)


def steps_of(key, shape, pieces, smallest, high):
    def one(dim, parts):
        draws = jax.random.uniform(jax.random.fold_in(jax.random.fold_in(key, 6), dim), (parts,), jnp.float32, smallest / len(pieces), high / len(pieces))
        return jnp.repeat(jnp.exp(draws), shape[dim] // parts).reshape((-1,) + (1,) * (len(shape) - dim - 1))

    loudness = one(*pieces[0])
    for cut in pieces[1:]:
        loudness = loudness * one(*cut)
    return loudness


def gaussian(key, extent, deviation, limit, shards=(), held_as=jnp.bfloat16):
    values = deviation * jax.random.normal(key, extent, jnp.float32)
    if shards:
        values = values * steps_of(key, extent, shards, -0.22, 0.18)
    return jnp.clip(values, -limit, limit).astype(held_as)


def setup_inputs(seed: int = 0) -> dict:
    arg_keys = jax.random.split(jax.random.key(seed), 10)
    tokens = gaussian(arg_keys[0], (TOKENS, D), 1.0, 6.0, ((0, 128),))
    routes = draw_routes(jax.random.fold_in(arg_keys[9], 71), 0)
    gates = jnp.clip(0.1 + 0.5 * jax.random.uniform(arg_keys[2], (TOKENS, TOPK), jnp.float32) ** steps_of(arg_keys[2], (TOKENS, TOPK), ((0, 128),), -0.2, 0.2), 0.1, 0.6)
    w_gate = gaussian(arg_keys[3], (EXPERTS, D, F), D ** -0.5, 0.125, ((0, 128),))
    w_up = gaussian(arg_keys[4], (EXPERTS, D, F), D ** -0.5, 0.125, ((0, 128),))
    w_down = gaussian(arg_keys[5], (EXPERTS, F, D), F ** -0.5, 0.21875, ((0, 128),))
    moe_out = draw_moe_out(jax.random.fold_in(arg_keys[9], 71), 0)
    norm_gain = jnp.clip(1.0 + 0.18 * jax.random.normal(arg_keys[7], (D,), jnp.float32), 0.1, 1.9)
    out_grad = draw_out_grad(jax.random.fold_in(arg_keys[9], 71), 0)
    return {"tokens": tokens, "routes": routes, "gates": gates, "w_gate": w_gate, "w_up": w_up, "w_down": w_down, "moe_out": moe_out, "norm_gain": norm_gain, "out_grad": out_grad}


epsilon = 1e-06
block_rows = 256

def contract(left, right, left_dim, right_dim):
    return lax.dot_general(left, right, (((left_dim,), (right_dim,)), ((), ())), preferred_element_type=jnp.float32)

def norm_backward(moe_out, norm_gain, out_grad):
    features = moe_out.shape[1]
    saved_out = moe_out.astype(jnp.float32)
    scaled = norm_gain.astype(jnp.float32)[None, :] * out_grad.astype(jnp.float32)
    square_sum = lax.optimization_barrier(jnp.sum(saved_out * saved_out, axis=1))
    cross_sum = lax.optimization_barrier(jnp.sum(saved_out * scaled, axis=1))
    inv_rms = lax.rsqrt(square_sum / features + epsilon)
    result = inv_rms[:, None] * scaled - saved_out * (inv_rms ** 3 * cross_sum / features)[:, None]
    return result.astype(jnp.bfloat16)

def expert_terms(row_block, cot_block, gate_row, w_gate_one, w_up_one, w_down_one):
    pre_gate = jnp.dot(row_block, w_gate_one, preferred_element_type=jnp.float32)
    pre_up = jnp.dot(row_block, w_up_one, preferred_element_type=jnp.float32)
    sigmoid_gate = jax.nn.sigmoid(pre_gate)
    activated = pre_gate * sigmoid_gate
    hidden = activated * pre_up
    hid_grad = contract(cot_block, w_down_one, 1, 1)
    gate_grad = lax.optimization_barrier(jnp.sum(hidden * hid_grad, axis=1)).astype(jnp.bfloat16)
    weight = gate_row.astype(jnp.float32)[:, None]
    d_hidden = weight * hid_grad
    d_gate = (d_hidden * pre_up * sigmoid_gate * (1.0 + pre_gate * (1.0 - sigmoid_gate))).astype(jnp.bfloat16)
    d_up = (d_hidden * activated).astype(jnp.bfloat16)
    token_back = (contract(d_gate, w_gate_one, 1, 1) + contract(d_up, w_up_one, 1, 1)).astype(jnp.bfloat16)
    scaled_cot = (weight * cot_block.astype(jnp.float32)).astype(jnp.bfloat16)
    grad_gate = contract(row_block, d_gate, 0, 0)
    grad_up = contract(row_block, d_up, 0, 0)
    grad_down = contract(hidden.astype(jnp.bfloat16), scaled_cot, 0, 0)
    return (token_back, gate_grad, grad_gate, grad_up, grad_down)

def reference(tokens, routes, gates, w_gate, w_up, w_down, moe_out, norm_gain, out_grad):
    features = tokens.shape[1]
    hidden_width = w_gate.shape[2]
    expert_cot = norm_backward(moe_out, norm_gain, out_grad)
    flat_ids = routes.reshape(-1).astype(jnp.int32)
    route_count = flat_ids.shape[0]
    flat_token = (jnp.arange(route_count, dtype=jnp.int32) // TOPK).astype(jnp.int32)
    flat_gate = gates.reshape(-1).astype(jnp.bfloat16)
    sorted_order = jnp.argsort(flat_ids, stable=True).astype(jnp.int32)
    totals = jnp.zeros((EXPERTS,), jnp.int32).at[flat_ids].add(1)
    starts = (jnp.cumsum(totals) - totals).astype(jnp.int32)
    token_pad = jnp.concatenate([tokens, jnp.zeros((1, features), jnp.bfloat16)], axis=0)
    cot_pad = jnp.concatenate([expert_cot, jnp.zeros((1, features), jnp.bfloat16)], axis=0)

    def per_expert(state_pair, inputs):
        expert_index, w_gate_one, w_up_one, w_down_one = inputs
        first_slot = starts[expert_index]
        load_size = totals[expert_index]

        def one_block(block_index, state):
            route_dx, route_gg, acc_gate, acc_up, acc_down = state
            position = (first_slot + block_index * block_rows + jnp.arange(block_rows, dtype=jnp.int32)).astype(jnp.int32)
            in_range = position < first_slot + load_size
            route_ids = sorted_order[jnp.clip(position, 0, route_count - 1)]
            token_ids = jnp.where(in_range, flat_token[route_ids], TOKENS).astype(jnp.int32)
            gate_row = jnp.where(in_range, flat_gate[route_ids], jnp.zeros((), jnp.bfloat16))
            target = jnp.where(in_range, route_ids, route_count).astype(jnp.int32)
            token_back, gate_grad, grad_gate, grad_up, grad_down = expert_terms(token_pad[token_ids], cot_pad[token_ids], gate_row, w_gate_one, w_up_one, w_down_one)
            route_dx = route_dx.at[target].set(token_back)
            route_gg = route_gg.at[target].set(gate_grad)
            return (route_dx, route_gg, acc_gate + grad_gate, acc_up + grad_up, acc_down + grad_down)
        blocks = (load_size + block_rows - 1) // block_rows
        start_state = (state_pair[0], state_pair[1], jnp.zeros((features, hidden_width), jnp.float32), jnp.zeros((features, hidden_width), jnp.float32), jnp.zeros((hidden_width, features), jnp.float32))
        route_dx, route_gg, acc_gate, acc_up, acc_down = lax.fori_loop(0, blocks, one_block, start_state)
        return ((route_dx, route_gg), (acc_gate.astype(jnp.bfloat16), acc_up.astype(jnp.bfloat16), acc_down.astype(jnp.bfloat16)))
    start_pair = (jnp.zeros((route_count + 1, features), jnp.bfloat16), jnp.zeros((route_count + 1,), jnp.bfloat16))
    final_pair, stacked = lax.scan(per_expert, start_pair, (jnp.arange(EXPERTS, dtype=jnp.int32), w_gate, w_up, w_down))
    route_dx, route_gg = final_pair
    token_grad = lax.optimization_barrier(jnp.sum(route_dx[:route_count].astype(jnp.float32).reshape(TOKENS, TOPK, features), axis=1)).astype(jnp.bfloat16)
    gates_grad = route_gg[:route_count].reshape(TOKENS, TOPK)
    return (token_grad, gates_grad, stacked[0], stacked[1], stacked[2])
```

```python
import math

import jax
import jax.numpy as jnp
from jax import lax
from jax.sharding import PartitionSpec as P

from jax.experimental import pallas as pl
from jax.experimental.pallas import tpu as pltpu

MESH = pl.DeviceIdType.MESH
SIZE = {"z": 4, "x": 4, "t": 8}
AXIS = {"z": 0, "x": 1, "t": 2}


def coords():
    ep = lax.axis_index("ep")
    return {"z": ep // 4, "x": ep % 4, "t": lax.axis_index("tp")}


def peers(dim, here):
    if dim != "t":
        return [(here + k) % 4 for k in (1, 3, 2)]
    return [
        (here // 2 + dy) % 4 * 2 + (here % 2 + dc) % 2
        for dy, dc in ((1, 0), (3, 0), (1, 1), (3, 1), (2, 0), (2, 1), (0, 1))
    ]


def device_of(place):
    return (place["z"] * 4 + place["x"], place["t"])


def barrier():
    me = coords()
    sem = pltpu.get_barrier_semaphore()
    count = 0
    for dim in "zxt":
        for p in peers(dim, me[dim]):
            count += 1
            pl.semaphore_signal(
                sem, inc=1, device_id=device_of({**me, dim: p}), device_id_type=MESH
            )
    pl.semaphore_wait(sem, count)


def cut(ref, dim, index):
    return ref.at[(slice(None),) * AXIS[dim] + (index,)]


def send(dim, src, dst, ssem, rsem, lsem):
    me = coords()
    for p in peers(dim, me[dim]):
        pltpu.make_async_remote_copy(
            cut(src, dim, p),
            cut(dst, dim, me[dim]),
            ssem,
            rsem,
            device_id=device_of({**me, dim: p}),
            device_id_type=MESH,
        ).start()
    pltpu.make_async_copy(cut(src, dim, me[dim]), cut(dst, dim, me[dim]), lsem).start()


def arrived(dim, dst, rsem, lsem):
    part = cut(dst, dim, slice(0, SIZE[dim] - 1))
    pltpu.make_async_copy(part, part, rsem).wait()
    one = cut(dst, dim, 0)
    pltpu.make_async_copy(one, one, lsem).wait()


def left(dim, src, ssem):
    part = cut(src, dim, slice(0, SIZE[dim] - 1))
    pltpu.make_async_copy(part, part, ssem).wait()


ROUNDS = (
    (0, "x"), (1, "t"), (2, "z"),
    (3, "x"), (0, "t"), (1, "z"),
    (2, "x"), (3, "t"), (0, "z"),
    (1, "x"), (2, "t"), (3, "z"),
)


def exchange_kernel(x_ref, o_ref, b1, b2, ssem, rsem, lsem):
    barrier()
    dims = {}
    for c, d in ROUNDS:
        k = len(dims.setdefault(c, []))
        bufs = (x_ref.at[c], b1.at[c], b2.at[c], o_ref.at[c])
        if k:
            arrived(dims[c][-1], bufs[k], rsem.at[c, k - 1], lsem.at[c, k - 1])
        send(d, bufs[k], bufs[k + 1], ssem.at[c, k], rsem.at[c, k], lsem.at[c, k])
        dims[c].append(d)
    for c in dims:
        bufs = (x_ref.at[c], b1.at[c], b2.at[c], o_ref.at[c])
        arrived(dims[c][2], bufs[3], rsem.at[c, 2], lsem.at[c, 2])
        for k in range(3):
            left(dims[c][k], bufs[k], ssem.at[c, k])


def exchange(rows, cid):
    shape = (4, 4, 4, 8, 16, 128)
    laid = rows.reshape(4, 4, 8, 4, 16, 128).transpose(3, 0, 1, 2, 4, 5)
    out = pl.pallas_call(
        exchange_kernel,
        out_shape=jax.ShapeDtypeStruct(shape, jnp.bfloat16),
        in_specs=[pl.BlockSpec(memory_space=pltpu.VMEM)],
        out_specs=pl.BlockSpec(memory_space=pltpu.VMEM),
        scratch_shapes=[
            pltpu.VMEM(shape, jnp.bfloat16),
            pltpu.VMEM(shape, jnp.bfloat16),
            pltpu.SemaphoreType.DMA((4, 3)),
            pltpu.SemaphoreType.DMA((4, 3)),
            pltpu.SemaphoreType.DMA((4, 3)),
        ],
        compiler_params=pltpu.CompilerParams(
            collective_id=cid, has_side_effects=True, vmem_limit_bytes=20 << 20
        ),
        name="exchange",
    )(laid)
    return out.transpose(1, 2, 3, 0, 4, 5).reshape(rows.shape)

epsilon = 1e-06


def from_everyone(value, axis):
    copies = jnp.broadcast_to(value, (lax.axis_size(axis), *value.shape))
    return lax.all_to_all(copies, axis, split_axis=0, concat_axis=0, tiled=True)


def over_copies(value, axis):
    everything = from_everyone(value, axis)
    return jnp.sum(everything, axis=0)


def packed_total(arrays, axis):
    ravelled, at, outs = (jnp.concatenate([a.reshape(-1) for a in arrays]), 0, [])
    running = over_copies(ravelled, axis)
    for a in arrays:
        outs.append(running[at : at + a.size].reshape(a.shape))
        at += a.size
    return tuple(outs)


def sent_together(arrays, axis, split_dim, concat_dim, along):
    widths = [math.prod(a.shape[along:]) for a in arrays]
    both = jnp.concatenate(
        [a.reshape(*a.shape[:along], w) for a, w in zip(arrays, widths)], axis=along
    )
    result = lax.all_to_all(both, axis, split_axis=split_dim, concat_axis=concat_dim, tiled=True)
    parts = jnp.split(result, [sum(widths[:k]) for k in range(1, len(widths))], axis=along)
    return tuple(
        (b.reshape(*result.shape[:along], *a.shape[along:]) for a, b in zip(arrays, parts))
    )


def contract(left, right, left_dim, right_dim):
    return lax.dot_general(
        left, right, (((left_dim,), (right_dim,)), ((), ())), preferred_element_type=jnp.float32
    )


def slot_ranks(flat_ids, experts):
    one_hot = (flat_ids[:, None] == jnp.arange(experts, dtype=jnp.int32)[None, :]).astype(jnp.int32)
    return jnp.sum((jnp.cumsum(one_hot, axis=0) - one_hot) * one_hot, axis=1)


def local(tokens, routes, gates, w_gate, w_up, w_down, moe_out, norm_gain, out_grad):
    devices = lax.axis_size(("ep", "tp"))
    tok_rows, features = tokens.shape
    top_count = routes.shape[1]
    capacity = 4 * tok_rows // devices
    route_count = tok_rows * top_count
    saved_out = moe_out.astype(jnp.float32)
    scaled = norm_gain[None, :] * out_grad.astype(jnp.float32)
    square_sum, cross_sum = packed_total(
        (jnp.sum(saved_out * saved_out, axis=1), jnp.sum(saved_out * scaled, axis=1)), "tp"
    )
    inv_rms = lax.rsqrt(square_sum / features + epsilon)
    expert_cot = (
        inv_rms[:, None] * scaled - saved_out * (inv_rms**3 * cross_sum / features)[:, None]
    ).astype(jnp.bfloat16)
    flat_ids = routes.reshape(-1)
    own_slots = flat_ids * capacity + slot_ranks(flat_ids, devices)
    route_tokens = jnp.arange(route_count, dtype=jnp.int32) // top_count
    token_of_slot = (
        jnp.full((devices * capacity,), tok_rows, jnp.int32).at[own_slots].set(route_tokens)
    )
    gate_slots = (
        jnp.zeros((devices * capacity,), jnp.bfloat16)
        .at[own_slots]
        .set(gates.reshape(-1).astype(jnp.bfloat16))
        .reshape(devices, capacity)
    )
    token_pad = jnp.concatenate([tokens, jnp.zeros((1, features), jnp.bfloat16)], axis=0)
    token_slots = token_pad[token_of_slot].reshape(devices, capacity, features)
    cot_rows = lax.all_to_all(expert_cot, "tp", split_axis=0, concat_axis=1, tiled=True)
    cot_pad = jnp.concatenate([cot_rows, jnp.zeros((1, features), jnp.bfloat16)], axis=0)
    cot_slots = cot_pad[token_of_slot].reshape(devices, capacity, features)
    token_in, cot_in, gate_in = (
        exchange(token_slots, 0),
        exchange(cot_slots, 0),
        lax.all_to_all(gate_slots, ("ep", "tp"), split_axis=0, concat_axis=0, tiled=True),
    )
    cot_in = cot_in.reshape(devices * capacity, features)
    row_block = token_in.reshape(devices * capacity, features)
    w_gate_one = w_gate[0]
    w_up_one = w_up[0]
    w_down_one = w_down[0]
    pre_gate = jnp.dot(row_block, w_gate_one, preferred_element_type=jnp.float32)
    pre_up = jnp.dot(row_block, w_up_one, preferred_element_type=jnp.float32)
    sigmoid_gate = jax.nn.sigmoid(pre_gate)
    activated = pre_gate * sigmoid_gate
    hidden = activated * pre_up
    hid_grad = contract(cot_in, w_down_one, 1, 1)
    gate_grad = jnp.sum(hidden * hid_grad, axis=1).astype(jnp.bfloat16)
    weight = gate_in.reshape(-1).astype(jnp.float32)[:, None]
    d_hidden = weight * hid_grad
    d_gate = (d_hidden * pre_up * sigmoid_gate * (1.0 + pre_gate * (1.0 - sigmoid_gate))).astype(
        jnp.bfloat16
    )
    d_up = (d_hidden * activated).astype(jnp.bfloat16)
    token_back = (contract(d_gate, w_gate_one, 1, 1) + contract(d_up, w_up_one, 1, 1)).astype(
        jnp.bfloat16
    )
    scaled_cot = (weight * cot_in.astype(jnp.float32)).astype(jnp.bfloat16)
    grad_gate = contract(row_block, d_gate, 0, 0).astype(jnp.bfloat16)
    grad_up = contract(row_block, d_up, 0, 0).astype(jnp.bfloat16)
    grad_down = contract(hidden.astype(jnp.bfloat16), scaled_cot, 0, 0).astype(jnp.bfloat16)
    back_rows = exchange(token_back.reshape(devices, capacity, features), 0)
    back_gates = lax.all_to_all(
        gate_grad.reshape(devices, capacity), ("ep", "tp"), split_axis=0, concat_axis=0, tiled=True
    )
    per_route = back_rows.reshape(devices * capacity, features)[own_slots]
    token_grad = jnp.sum(
        per_route.astype(jnp.float32).reshape(tok_rows, top_count, features), axis=1
    ).astype(jnp.bfloat16)
    gates_grad = back_gates.reshape(-1)[own_slots].reshape(tok_rows, top_count)
    return (token_grad, gates_grad, grad_gate[None], grad_up[None], grad_down[None])


def solution(mesh):
    in_specs = (
        P(("ep", "tp"), None),
        P(("ep", "tp"), None),
        P(("ep", "tp"), None),
        P(("ep", "tp"), None, None),
        P(("ep", "tp"), None, None),
        P(("ep", "tp"), None, None),
        P("ep", "tp"),
        P("tp"),
        P("ep", "tp"),
    )
    out_specs = (
        P(("ep", "tp"), None),
        P(("ep", "tp"), None),
        P(("ep", "tp"), None, None),
        P(("ep", "tp"), None, None),
        P(("ep", "tp"), None, None),
    )
    return jax.shard_map(local, mesh=mesh, in_specs=in_specs, out_specs=out_specs, check_vma=False)
```

```python
import jax
import jax.numpy as jnp
from jax import lax
from jax.experimental import pallas as pl
from jax.experimental.pallas import tpu as pltpu
from jax.sharding import PartitionSpec as P

F32 = jnp.float32
BF16 = jnp.bfloat16
MESH = pl.DeviceIdType.MESH
VMEM = pl.BlockSpec(memory_space=pltpu.VMEM)
SMEM = pl.BlockSpec(memory_space=pltpu.SMEM)
ANY = pl.BlockSpec(memory_space=pl.ANY)
SIZE = {"z": 4, "x": 4, "t": 8}
AXIS = {"z": 0, "x": 1, "t": 2}
epsilon = 1e-06

PLAN = (
    "bar", "T1t", "T0x", "stat", "T7x", "T4z", "T5z", "T2t", "cot", "T3x", "T1z", "T4x",
    "T7z", "T0z", "T2x", "T6t", "T1x", "T5t", "T3z", "table", "C0t", "C1x", "T4t", "C3t",
    "T2z", "C2x", "C4z", "C7x", "T3t", "C1z", "C0x", "C6t", "C2z", "T0t", "T5x", "C3z",
    "C5x", "C1t", "T6z", "C0z", "C6x", "C2t", "A1", "C3x", "C4x", "A2", "T6x", "C7z",
    "C5t", "T7t", "A0", "C6z", "B0", "D0", "R1z", "C7t", "B1", "C5z", "R2x", "R0x",
    "C4t", "D1", "R3z", "A3", "R1t", "B3", "R6z", "R2t", "B2", "R4z", "R0t", "R1x",
    "D2", "R3x", "R5z", "D3", "R7t", "R6x", "R2z", "R4t", "R5x", "R7z", "R3t", "R0z",
    "R6t", "R4x", "R7x", "R5t",
)


def iota(shape, dim):
    return lax.broadcasted_iota(jnp.int32, shape, dim)


def dot(a, b, a_dim=1, b_dim=0):
    return lax.dot_general(
        a, b, (((a_dim,), (b_dim,)), ((), ())), preferred_element_type=F32
    )


def to_rows():
    i, j = iota((256, 256), 0), iota((256, 256), 1)
    return (((i >> 5) == (j & 7)) & ((i & 31) == (j >> 3))).astype(F32).astype(BF16)


def to_tiles():
    i, j = iota((256, 256), 0), iota((256, 256), 1)
    return (((i >> 3) == (j & 31)) & ((i & 7) == (j >> 5))).astype(F32).astype(BF16)


def tile_pair(perm, pieces, put):
    for pair in range(2):
        both = jnp.concatenate(
            [jnp.concatenate(pieces(2 * pair + j), axis=0) for j in range(2)], axis=1
        )
        out = dot(perm, both).astype(BF16)
        for j in range(2):
            put(2 * pair + j, out[:, 128 * j : 128 * (j + 1)])


def row_pair(perm, tiles, put):
    for pair in range(2):
        both = jnp.concatenate([tiles(2 * pair + j) for j in range(2)], axis=1)
        out = dot(perm, both).astype(BF16)
        for j in range(2):
            for b in range(8):
                put(2 * pair + j, b, out[32 * b : 32 * (b + 1), 128 * j : 128 * (j + 1)])


def route_kernel(
    routes_ref, gates_ref, tokens_ref, moe_ref, grad_ref, gain_ref,
    index_ref, spot_ref, gate_ref, pick_ref, table_ref, stat_ref,
):
    head = jnp.concatenate(
        [routes_ref[...].astype(F32), gates_ref[...], jnp.zeros((4, 128), F32)], axis=0
    )
    cols = head.T
    lane, row = iota((128, 128), 1), iota((128, 128), 0)
    lane_f = lane.astype(F32)
    below = (lane < row).astype(F32).astype(BF16)
    hot = [(cols[:, k : k + 1] == lane_f).astype(F32) for k in range(2)]
    seen = dot(below, (hot[0] + hot[1]).astype(BF16))
    rank = [jnp.sum(hot[k] * seen, axis=1, keepdims=True) for k in range(2)]
    number = (row + 1).astype(F32)
    index = jnp.zeros((128, 128), F32)
    gate = jnp.zeros((128, 128), F32)
    for k in range(2):
        at = lane_f == rank[k]
        one = hot[k].astype(BF16)
        index += dot(jnp.where(at, number, 0.0).astype(BF16), one, 0, 0)
        gate += dot(one, jnp.where(at, cols[:, 2 + k : 3 + k], 0.0).astype(BF16), 0, 0)
    index_ref[...] = index[:8].astype(jnp.int32)
    gate_ref[:, 0, :] = gate
    pick = jnp.zeros((128, 128), F32)
    for k in range(2):
        pick = jnp.where(lane == k, rank[k] * 256.0 + cols[:, k : k + 1], pick)
        pick = jnp.where(lane == 2 + k, cols[:, k : k + 1], pick)
        pick = jnp.where(lane == 4 + k, rank[k], pick)
    pick_ref[...] = pick
    spot_ref[...] = pick.T[:8].astype(jnp.int32)
    perm = to_tiles()
    for h in range(2):
        table_ref[h, 0] = jnp.zeros((8, 128), BF16)

        def pieces(g, h=h):
            return [
                tokens_ref[32 * g : 32 * (g + 1), 1024 * h + 128 * b : 1024 * h + 128 * (b + 1)]
                for b in range(8)
            ]

        def put(g, tiles, h=h):
            table_ref[h, 1 + 32 * g : 33 + 32 * g] = tiles.reshape(32, 8, 128)

        tile_pair(perm, pieces, put)
    for b in range(8):
        saved = moe_ref[128 * b : 128 * (b + 1), :].astype(F32)
        scaled = gain_ref[...] * grad_ref[128 * b : 128 * (b + 1), :].astype(F32)
        for s, prod in enumerate((saved * saved, saved * scaled)):
            part = (prod[:, :128] + prod[:, 128:]).T
            stat_ref[s, b : b + 1, :] = jnp.sum(part, axis=0, keepdims=True)


def coords():
    ep = lax.axis_index("ep")
    return {"z": ep // 4, "x": ep % 4, "t": lax.axis_index("tp")}


def peers(dim, here):
    if dim != "t":
        return [(here + k) % 4 for k in (1, 3, 2)]
    return [
        (here // 2 + dy) % 4 * 2 + (here % 2 + dc) % 2
        for dy, dc in ((1, 0), (3, 0), (1, 1), (3, 1), (2, 0), (2, 1), (0, 1))
    ]


def others():
    me = coords()
    for dim in "zxt":
        for p in peers(dim, me[dim]):
            place = {**me, dim: p}
            yield dim, p, (place["z"] * 4 + place["x"], place["t"])


def greet():
    for _, _, device in others():
        pl.semaphore_signal(
            pltpu.get_barrier_semaphore(), inc=1, device_id=device, device_id_type=MESH
        )


def cut(ref, axis, index):
    return ref.at[(slice(None),) * axis + (index,)]


class Hop:
    def __init__(self, dim, axis, src, dst, sems, whole=False):
        self.dim, self.axis, self.whole = dim, axis, whole
        self.src, self.dst, (self.ssem, self.rsem, self.lsem) = src, dst, sems

    def piece(self, index):
        return self.src if self.whole else cut(self.src, self.axis, index)

    def start(self):
        mine = coords()[self.dim]
        for dim, p, device in others():
            if dim == self.dim:
                pltpu.make_async_remote_copy(
                    self.piece(p),
                    cut(self.dst, self.axis, mine),
                    self.ssem,
                    self.rsem,
                    device_id=device,
                    device_id_type=MESH,
                ).start()
        pltpu.make_async_copy(self.piece(mine), cut(self.dst, self.axis, mine), self.lsem).start()

    def remote_part(self):
        return cut(self.dst, self.axis, slice(0, SIZE[self.dim] - 1))

    def arrived(self):
        part = self.remote_part()
        pltpu.make_async_copy(part, part, self.rsem).wait()
        one = cut(self.dst, self.axis, 0)
        pltpu.make_async_copy(one, one, self.lsem).wait()

    def left(self):
        part = self.remote_part()
        pltpu.make_async_copy(part, part, self.ssem).wait()


def pack(index_ref, rank, table_ref, half, dst):
    def body(i, carry):
        for t in range(8):
            dst[i // 4, i % 4, t] = table_ref[half, index_ref[rank, i * 8 + t]]
        return carry

    lax.fori_loop(0, 16, body, 0)


def mega_kernel(
    index_ref, gate_ref, table_ref, stat_ref, moe_ref, grad_ref, gain_ref, wg_any, wu_any, wd_any,
    back_ref, slope_ref, x_rows, d_gate, d_up, hidden, scaled_cot,
    wg, wu, wd, t_src, t_one, t_two, t_out, c_src, c_one, c_two, c_out, r_src, r_one, r_two,
    g_one, g_two, g_out, q_src, q_one, q_two, s_in, cot_out, cot_in, cot_table,
    pre_gate, pre_up, cot_rows, back_rows, slope,
    ssem, rsem, lsem, misc, wsem,
):
    greet()
    weights = [
        pltpu.make_async_copy(a, b, wsem.at[i])
        for i, (a, b) in enumerate(((wg_any, wg), (wu_any, wu), (wd_any, wd)))
    ]
    for w in weights:
        w.start()
    slope[...] = jnp.zeros((128, 128), F32)
    unpack_perm, pack_perm = to_rows(), to_tiles()
    families = {
        "T": (t_src, t_one, t_two, t_out),
        "C": (c_src, c_one, c_two, c_out),
        "R": (r_src, r_one, r_two, back_ref),
    }
    hops = {}
    every = []

    def small(i):
        return tuple(misc.at[i, j] for j in range(3))

    stat_hop = Hop("t", 0, stat_ref, s_in, small(0), whole=True)
    cot_hop = Hop("t", 0, cot_out, cot_in, small(1))
    gate_hops = [
        Hop(d, AXIS[d], a, b, small(2 + i))
        for i, (d, a, b) in enumerate(
            (("x", gate_ref, g_one), ("t", g_one, g_two), ("z", g_two, g_out))
        )
    ]
    slope_hops = [
        Hop(d, AXIS[d], a, b, small(5 + i))
        for i, (d, a, b) in enumerate(
            (("x", q_src, q_one), ("t", q_one, q_two), ("z", q_two, slope_ref))
        )
    ]

    def begin(hop):
        hop.start()
        every.append(hop)

    def norm_statistics():
        begin(stat_hop)
        begin(gate_hops[0])

    def cotangents():
        stat_hop.arrived()
        total = s_in[0]
        for p in range(1, 8):
            total += s_in[p]
        inv = lax.rsqrt(total[0] / 2048.0 + epsilon)
        cols = jnp.concatenate([inv, inv**3 * total[1] / 2048.0], axis=0).T

        for b in range(8):
            rows = slice(128 * b, 128 * (b + 1))
            scaled = gain_ref[...] * grad_ref[rows, :].astype(F32)
            saved = moe_ref[rows, :].astype(F32)
            cot_out[b] = (
                cols[:, b : b + 1] * scaled - saved * cols[:, 8 + b : 9 + b]
            ).astype(BF16)
        begin(cot_hop)
        gate_hops[0].arrived()
        begin(gate_hops[1])

    def cotangent_table():
        cot_hop.arrived()
        for h in range(2):
            cot_table[h, 0] = jnp.zeros((8, 128), BF16)

            def pieces(g, h=h):
                return [
                    cot_in[4 * h + b // 2, 32 * g : 32 * (g + 1), b % 2 * 128 : b % 2 * 128 + 128]
                    for b in range(8)
                ]

            def put(g, tiles, h=h):
                cot_table[h, 1 + 32 * g : 33 + 32 * g] = tiles.reshape(32, 8, 128)

            tile_pair(pack_perm, pieces, put)
        gate_hops[1].arrived()
        begin(gate_hops[2])

    def unpack(src, dst, row, half):
        def put(g, b, rows):
            dst[
                row + 32 * g : row + 32 * (g + 1), 1024 * half + 128 * b : 1024 * half + 128 * b + 128
            ] = rows

        row_pair(unpack_perm, lambda g: src[g].reshape(256, 128), put)

    def hidden_inputs(r):
        if r == 1:
            weights[0].wait()
            weights[1].wait()
        for h in range(2):
            hops["T", 2 * r + h][2].arrived()
            unpack(t_out.at[2 * r + h], x_rows, 128 * r, h)

        def body(n, carry):
            cols = pl.ds(pl.multiple_of(n * 256, 256), 256)
            x = x_rows[128 * r : 128 * (r + 1), :]
            pre_gate[r, :, cols] = dot(x, wg[:, cols])
            pre_up[r, :, cols] = dot(x, wu[:, cols])
            return carry

        lax.fori_loop(0, 3, body, 0)

    def half_back(r, h):
        rows = slice(128 * r, 128 * (r + 1))

        def body(n, carry):
            wide = pl.ds(pl.multiple_of(1024 * h + n * 256, 256), 256)
            total = dot(d_gate[rows, :], wg[wide, :], 1, 1) + dot(d_up[rows, :], wu[wide, :], 1, 1)
            back_rows[:, pl.ds(pl.multiple_of(n * 256, 256), 256)] = total.astype(BF16)
            return carry

        lax.fori_loop(0, 4, body, 0)

        def pieces(g):
            return [
                back_rows[32 * g : 32 * (g + 1), 128 * b : 128 * (b + 1)] for b in range(8)
            ]

        def put(g, tiles):
            r_src[2 * r + h, g] = tiles.reshape(4, 8, 8, 128)

        tile_pair(pack_perm, pieces, put)

    def slopes(r):
        if r == 0:
            weights[2].wait()
            gate_hops[2].arrived()
        for h in range(2):
            hops["C", 2 * r + h][2].arrived()
            unpack(c_out.at[2 * r + h], cot_rows, 0, h)
        gates = jnp.concatenate(
            [g_out[z, x][:, 0, :] for z in range(4) for x in range(4)], axis=0
        )
        gate = gates[:, r : r + 1]
        rows = slice(128 * r, 128 * (r + 1))

        def body(n, carry):
            cols = pl.ds(pl.multiple_of(n * 256, 256), 256)
            hid_grad = dot(cot_rows[...], wd[cols, :], 1, 1)
            p_gate, p_up = pre_gate[r, :, cols], pre_up[r, :, cols]
            sig = jax.nn.sigmoid(p_gate)
            act = p_gate * sig
            hid = act * p_up
            d_hid = gate * hid_grad
            d_gate[rows, cols] = (d_hid * p_up * sig * (1.0 + p_gate * (1.0 - sig))).astype(BF16)
            d_up[rows, cols] = (d_hid * act).astype(BF16)
            hidden[rows, cols] = hid.astype(BF16)
            return carry + jnp.sum(hid * hid_grad, axis=1, keepdims=True)

        total = lax.fori_loop(0, 3, body, jnp.zeros((128, 1), F32))
        slope[...] = jnp.where(iota((128, 128), 1) == r, total, slope[...])
        scaled_cot[rows, :] = (gate * cot_rows[...].astype(F32)).astype(BF16)
        half_back(r, 0)

    def rest(r):
        half_back(r, 1)
        if r == 3:
            for z in range(4):
                for x in range(4):
                    q_src[z, x, :, 0, :] = slope[32 * z + 8 * x : 32 * z + 8 * x + 8, :]
            begin(slope_hops[0])

    lasts = [i for i, step in enumerate(PLAN) if step[0] == "R"][-2:]
    for i, step in enumerate(PLAN):
        kind = step[0]
        if step == "bar":
            pl.semaphore_wait(pltpu.get_barrier_semaphore(), 13)
        elif step == "stat":
            norm_statistics()
        elif step == "cot":
            cotangents()
        elif step == "table":
            cotangent_table()
        elif kind == "A":
            hidden_inputs(int(step[1]))
        elif kind == "B":
            slopes(int(step[1]))
        elif kind == "D":
            rest(int(step[1]))
        else:
            c, d = int(step[1]), step[2]
            done = hops.setdefault((kind, c), [])
            k = len(done)
            bufs = families[kind]
            if k:
                done[-1].arrived()
            elif kind == "T":
                pack(index_ref, c // 2, table_ref, c % 2, t_src.at[c])
            elif kind == "C":
                pack(index_ref, c // 2, cot_table, c % 2, c_src.at[c])
            n = "TCR".index(kind) * 8 + c
            hop = Hop(
                d, AXIS[d], bufs[k].at[c], bufs[k + 1].at[c],
                (ssem.at[n, k], rsem.at[n, k], lsem.at[n, k]),
            )
            begin(hop)
            done.append(hop)
            if i == lasts[0]:
                slope_hops[0].arrived()
                begin(slope_hops[1])
    slope_hops[1].arrived()
    begin(slope_hops[2])
    for c in range(8):
        hops["R", c][2].arrived()
    slope_hops[2].arrived()
    for hop in every:
        hop.left()


def finish_kernel(spot_ref, back_ref, slope_ref, pick_ref, token_ref, gates_ref, sums):
    def body(i, carry):
        for j in range(8):
            t = i * 8 + j
            for h in range(2):
                one = back_ref[spot_ref[0, t] + 128 * h].astype(F32)
                two = back_ref[spot_ref[1, t] + 128 * h].astype(F32)
                sums[h, t] = (one + two).astype(BF16)
        return carry

    lax.fori_loop(0, 16, body, 0)
    perm = to_rows()
    for h in range(2):

        def put(g, b, rows, h=h):
            token_ref[32 * g : 32 * (g + 1), 1024 * h + 128 * b : 1024 * h + 128 * (b + 1)] = rows

        row_pair(perm, lambda g, h=h: sums[h, 32 * g : 32 * (g + 1)].reshape(256, 128), put)
    slope = slope_ref[:, 0, :].astype(BF16)
    pick = pick_ref[...]
    lane = iota((128, 128), 1)
    lane_f = lane.astype(F32)
    both = jnp.zeros((128, 128), F32)
    for k in range(2):
        one = (pick[:, 2 + k : 3 + k] == lane_f).astype(F32).astype(BF16)
        mine = jnp.where(lane_f == pick[:, 4 + k : 5 + k], dot(one, slope), 0.0)
        both = jnp.where(lane == k, jnp.sum(mine, axis=1, keepdims=True), both)
    gates_ref[...] = both.T[:2].astype(BF16)


def struct(shape, dtype=BF16):
    return jax.ShapeDtypeStruct(shape, dtype)


def local(tokens, routes, gates, w_gate, w_up, w_down, moe_out, norm_gain, out_grad):
    gain = norm_gain.reshape(1, 256)
    index, spot, gate, pick, table, stat = pl.pallas_call(
        route_kernel,
        out_shape=(
            struct((8, 128), jnp.int32),
            struct((8, 128), jnp.int32),
            struct((128, 1, 128), F32),
            struct((128, 128), F32),
            struct((2, 129, 8, 128)),
            struct((2, 8, 128), F32),
        ),
        in_specs=[VMEM] * 6,
        out_specs=(VMEM,) * 6,
        name="route",
    )(routes.T, gates.T, tokens, moe_out, out_grad, gain)
    pieces = (8, 4, 4, 8, 8, 128)
    lanes = (4, 4, 8, 1, 128)
    back, slope, x_rows, d_gate, d_up, hidden, scaled_cot = pl.pallas_call(
        mega_kernel,
        out_shape=(
            struct(pieces),
            struct(lanes, F32),
            struct((512, 2048)),
            struct((512, 768)),
            struct((512, 768)),
            struct((512, 768)),
            struct((512, 2048)),
        ),
        in_specs=[SMEM] + [VMEM] * 6 + [ANY] * 3,
        out_specs=(VMEM,) * 7,
        scratch_shapes=[
            pltpu.VMEM((2048, 768), BF16),
            pltpu.VMEM((2048, 768), BF16),
            pltpu.VMEM((768, 2048), BF16),
            *[pltpu.VMEM(pieces, BF16)] * 11,
            *[pltpu.VMEM(lanes, F32)] * 6,
            pltpu.VMEM((8, 2, 8, 128), F32),
            pltpu.VMEM((8, 128, 256), BF16),
            pltpu.VMEM((8, 128, 256), BF16),
            pltpu.VMEM((2, 129, 8, 128), BF16),
            pltpu.VMEM((4, 128, 768), F32),
            pltpu.VMEM((4, 128, 768), F32),
            pltpu.VMEM((128, 2048), BF16),
            pltpu.VMEM((128, 1024), BF16),
            pltpu.VMEM((128, 128), F32),
            pltpu.SemaphoreType.DMA((24, 3)),
            pltpu.SemaphoreType.DMA((24, 3)),
            pltpu.SemaphoreType.DMA((24, 3)),
            pltpu.SemaphoreType.DMA((8, 3)),
            pltpu.SemaphoreType.DMA((3,)),
        ],
        compiler_params=pltpu.CompilerParams(
            collective_id=0, has_side_effects=True, vmem_limit_bytes=62 << 20
        ),
        name="exchange",
    )(index, gate.reshape(lanes), table, stat, moe_out, out_grad, gain, w_gate[0], w_up[0], w_down[0])
    token_grad, gates_grad = pl.pallas_call(
        finish_kernel,
        out_shape=(struct((128, 2048)), struct((2, 128))),
        in_specs=[SMEM] + [VMEM] * 3,
        out_specs=(VMEM,) * 2,
        scratch_shapes=[pltpu.VMEM((2, 128, 8, 128), BF16)],
        name="finish",
    )(spot, back.reshape(1024, 8, 128), slope.reshape(128, 1, 128), pick)
    grads = [
        dot(a, b, 0, 0).astype(BF16)[None]
        for a, b in ((x_rows, d_gate), (x_rows, d_up), (hidden, scaled_cot))
    ]
    return (token_grad, gates_grad.T, *grads)


def solution(mesh):
    split = P(("ep", "tp"), None)
    expert = P(("ep", "tp"), None, None)
    in_specs = (split, split, split, expert, expert, expert, P("ep", "tp"), P("tp"), P("ep", "tp"))
    out_specs = (split, split, expert, expert, expert)
    return jax.shard_map(local, mesh=mesh, in_specs=in_specs, out_specs=out_specs, check_vma=False)
```

```python
import jax
import jax.numpy as jnp
from jax import lax
from jax.experimental import pallas as pl
from jax.experimental.pallas import tpu as pltpu
from jax.sharding import PartitionSpec as P

F32 = jnp.float32
BF16 = jnp.bfloat16
MESH = pl.DeviceIdType.MESH
VMEM = pl.BlockSpec(memory_space=pltpu.VMEM)
SMEM = pl.BlockSpec(memory_space=pltpu.SMEM)
ANY = pl.BlockSpec(memory_space=pl.ANY)
SIZE = {"z": 4, "x": 4, "t": 8}
AXIS = {"z": 0, "x": 1, "t": 2}
epsilon = 1e-06

PLAN = (
    "bar", "stat", "T7z", "T2x", "T0t", "T1x", "T5x", "T6z", "cot", "M0", "M2", "T3z",
    "T4x", "T1t", "T6x", "T2t", "T0z", "table", "C0z", "C1t", "C5z", "T0x", "C3x", "C2z",
    "C6t", "C7z", "T1z", "C0t", "C1x", "T3t", "C6x", "C2t", "C3t", "C1z", "C0x", "C7x",
    "T7t", "C4z", "T4t", "M1", "T3x", "A0", "T6t", "T2z", "C3z", "T5z", "C2x", "B0",
    "C5t", "T7x", "C4x", "D0", "R1x", "A1", "C6z", "T4z", "R0x", "C7t", "B1", "R2z",
    "T5t", "A3", "C4t", "D1", "R3t", "C5x", "B3", "R1z", "D3", "R7x", "R0z", "R6t",
    "R2t", "A2", "B2", "R4t", "D2", "R5x", "R7z", "S0", "R6x", "R0t", "R3z", "S3",
    "W0", "W4", "R1t", "S1", "W1", "S2", "W9", "R4x", "R5z", "R2x", "R7t", "W10",
    "W8", "W6", "R6z", "R3x", "R4z", "R5t", "W7", "W2", "W5", "W3",
)


def iota(shape, dim):
    return lax.broadcasted_iota(jnp.int32, shape, dim)


def dot(a, b, a_dim=1, b_dim=0):
    return lax.dot_general(
        a, b, (((a_dim,), (b_dim,)), ((), ())), preferred_element_type=F32
    )


def to_rows():
    i, j = iota((256, 256), 0), iota((256, 256), 1)
    return (((i >> 5) == (j & 7)) & ((i & 31) == (j >> 3))).astype(F32).astype(BF16)


def to_tiles():
    i, j = iota((256, 256), 0), iota((256, 256), 1)
    return (((i >> 3) == (j & 31)) & ((i & 7) == (j >> 5))).astype(F32).astype(BF16)


def tile_pair(perm, pieces, put):
    for pair in range(2):
        both = jnp.concatenate(
            [jnp.concatenate(pieces(2 * pair + j), axis=0) for j in range(2)], axis=1
        )
        out = dot(perm, both).astype(BF16)
        for j in range(2):
            put(2 * pair + j, out[:, 128 * j : 128 * (j + 1)])


def row_pair(perm, tiles, put):
    for pair in range(2):
        both = jnp.concatenate([tiles(2 * pair + j) for j in range(2)], axis=1)
        out = dot(perm, both).astype(BF16)
        for j in range(2):
            for b in range(8):
                put(2 * pair + j, b, out[32 * b : 32 * (b + 1), 128 * j : 128 * (j + 1)])


def statistics(moe, grad, gain_ref, stat_ref):
    for b in range(8):
        rows = slice(128 * b, 128 * (b + 1))
        saved = moe[rows, :].astype(F32)
        scaled = gain_ref[...] * grad[rows, :].astype(F32)
        for s, prod in enumerate((saved * saved, saved * scaled)):
            part = (prod[:, :128] + prod[:, 128:]).T
            stat_ref[s, b : b + 1, :] = jnp.sum(part, axis=0, keepdims=True)


def routing(routes_ref, gates_ref, index_ref, spot_ref, gate_ref, pick_ref):
    head = jnp.concatenate(
        [routes_ref[...].astype(F32), gates_ref[...], jnp.zeros((4, 128), F32)], axis=0
    )
    cols = head.T
    lane, row = iota((128, 128), 1), iota((128, 128), 0)
    lane_f = lane.astype(F32)
    below = (lane < row).astype(F32).astype(BF16)
    hot = [(cols[:, k : k + 1] == lane_f).astype(F32) for k in range(2)]
    seen = dot(below, (hot[0] + hot[1]).astype(BF16))
    rank = [jnp.sum(hot[k] * seen, axis=1, keepdims=True) for k in range(2)]
    number = (row + 1).astype(F32)
    index = jnp.zeros((128, 128), F32)
    gate = jnp.zeros((128, 128), F32)
    for k in range(2):
        at = lane_f == rank[k]
        one = hot[k].astype(BF16)
        index += dot(jnp.where(at, number, 0.0).astype(BF16), one, 0, 0)
        gate += dot(one, jnp.where(at, cols[:, 2 + k : 3 + k], 0.0).astype(BF16), 0, 0)
    index_ref[...] = jnp.clip(index[:8].astype(jnp.int32), 0, 128)
    for z in range(4):
        for x in range(4):
            gate_ref[z, x, :, 0, :] = gate[32 * z + 8 * x : 32 * z + 8 * x + 8, :]
    pick = jnp.zeros((128, 128), F32)
    for k in range(2):
        pick = jnp.where(lane == k, rank[k] * 256.0 + cols[:, k : k + 1], pick)
        pick = jnp.where(lane == 2 + k, cols[:, k : k + 1], pick)
        pick = jnp.where(lane == 4 + k, rank[k], pick)
    pick_ref[...] = pick
    spot_ref[...] = pick.T[:8].astype(jnp.int32)


def token_table(perm, tokens, table_ref):
    for h in range(2):
        table_ref[h, 0] = jnp.zeros((8, 128), BF16)

        def pieces(g, h=h):
            return [
                tokens[32 * g : 32 * (g + 1), 1024 * h + 128 * b : 1024 * h + 128 * (b + 1)]
                for b in range(8)
            ]

        def put(g, tiles, h=h):
            table_ref[h, 1 + 32 * g : 33 + 32 * g] = tiles.reshape(32, 8, 128)

        tile_pair(perm, pieces, put)


def coords():
    ep = lax.axis_index("ep")
    return {"z": ep // 4, "x": ep % 4, "t": lax.axis_index("tp")}


def peers(dim, here):
    if dim != "t":
        return [(here + k) % 4 for k in (1, 3, 2)]
    return [
        (here // 2 + dy) % 4 * 2 + (here % 2 + dc) % 2
        for dy, dc in ((1, 0), (3, 0), (1, 1), (3, 1), (2, 0), (2, 1), (0, 1))
    ]


def others():
    me = coords()
    for dim in "zxt":
        for p in peers(dim, me[dim]):
            place = {**me, dim: p}
            yield dim, p, (place["z"] * 4 + place["x"], place["t"])


def greet():
    for _, _, device in others():
        pl.semaphore_signal(
            pltpu.get_barrier_semaphore(), inc=1, device_id=device, device_id_type=MESH
        )


def cut(ref, axis, index):
    return ref.at[(slice(None),) * axis + (index,)]


class Hop:
    def __init__(self, dim, axis, src, dst, sems, whole=False):
        self.dim, self.axis, self.whole, self.gone = dim, axis, whole, False
        self.src, self.dst, (self.ssem, self.rsem, self.lsem) = src, dst, sems

    def piece(self, index):
        return self.src if self.whole else cut(self.src, self.axis, index)

    def start(self):
        mine = coords()[self.dim]
        for dim, p, device in others():
            if dim == self.dim:
                pltpu.make_async_remote_copy(
                    self.piece(p),
                    cut(self.dst, self.axis, mine),
                    self.ssem,
                    self.rsem,
                    device_id=device,
                    device_id_type=MESH,
                ).start()
        pltpu.make_async_copy(self.piece(mine), cut(self.dst, self.axis, mine), self.lsem).start()

    def remote_part(self):
        return cut(self.dst, self.axis, slice(0, SIZE[self.dim] - 1))

    def arrived(self):
        part = self.remote_part()
        pltpu.make_async_copy(part, part, self.rsem).wait()
        one = cut(self.dst, self.axis, 0)
        pltpu.make_async_copy(one, one, self.lsem).wait()

    def left(self):
        if self.gone:
            return
        self.gone = True
        part = self.remote_part()
        pltpu.make_async_copy(part, part, self.ssem).wait()


def pack(index_ref, rank, table_ref, half, dst):
    def body(i, carry):
        for t in range(8):
            dst[i // 4, i % 4, t] = table_ref[half, index_ref[rank, i * 8 + t]]
        return carry

    lax.fori_loop(0, 16, body, 0)


def mega_kernel(
    routes_ref, gates_ref, gain_ref, tokens_any, moe_any, grad_any, wg_any, wu_any, wd_any,
    back_ref, slope_ref, spot_ref, pick_ref, gate_grad, up_grad, down_grad,
    tokens, moe, grad, index_v, index_ref, gate_src, table_ref, stat_ref,
    wg_t, wu_t, wd_t, t_src, t_one, t_two, t_out, c_src, c_one, c_two, c_out, r_one, r_two,
    g_one, g_two, g_out, q_src, q_one, q_two, s_in, cot_out, cot_in, cot_table,
    x_rows, x_t, d_gate, d_up, hidden, pre_gate, pre_up, cot_rows, back_rows, slope,
    ssem, rsem, lsem, misc, wsem,
):
    wg, wu = gate_grad, up_grad
    loads = [
        pltpu.make_async_copy(a, b, wsem.at[i])
        for i, (a, b) in enumerate(
            (
                (moe_any, moe), (grad_any, grad), (tokens_any, tokens),
                (wg_any, gate_grad), (wu_any, up_grad), (wd_any, down_grad),
            )
        )
    ]
    loaded = set()

    def need(*which):
        for i in which:
            if i not in loaded:
                loads[i].wait()
                loaded.add(i)

    for load in loads:
        load.start()
    greet()
    slope[...] = jnp.zeros((128, 128), F32)
    unpack_perm, pack_perm = to_rows(), to_tiles()
    routing(routes_ref, gates_ref, index_v, spot_ref, gate_src, pick_ref)
    index_copy = pltpu.make_async_copy(index_v, index_ref, wsem.at[6])
    index_copy.start()
    need(0, 1)
    statistics(moe, grad, gain_ref, stat_ref)
    need(2)
    token_table(pack_perm, tokens, table_ref)
    index_copy.wait()
    families = {
        "T": (t_src, t_one, t_two, t_out),
        "C": (c_src, c_one, c_two, c_out),
        "R": (t_src, r_one, r_two, back_ref),
    }
    hops = {}
    every = []

    def small(i):
        return tuple(misc.at[i, j] for j in range(3))

    stat_hop = Hop("t", 0, stat_ref, s_in, small(0), whole=True)
    cot_hop = Hop("t", 0, cot_out, cot_in, small(1))
    gate_hops = [
        Hop(d, AXIS[d], a, b, small(2 + i))
        for i, (d, a, b) in enumerate(
            (("x", gate_src, g_one), ("t", g_one, g_two), ("z", g_two, g_out))
        )
    ]
    slope_hops = [
        Hop(d, AXIS[d], a, b, small(5 + i))
        for i, (d, a, b) in enumerate(
            (("x", q_src, q_one), ("t", q_one, q_two), ("z", q_two, slope_ref))
        )
    ]

    def begin(hop):
        hop.start()
        every.append(hop)

    def norm_statistics():
        begin(stat_hop)
        begin(gate_hops[0])

    def cotangents():
        stat_hop.arrived()
        total = s_in[0]
        for p in range(1, 8):
            total += s_in[p]
        inv = lax.rsqrt(total[0] / 2048.0 + epsilon)
        cols = jnp.concatenate([inv, inv**3 * total[1] / 2048.0], axis=0).T

        for b in range(8):
            rows = slice(128 * b, 128 * (b + 1))
            scaled = gain_ref[...] * grad[rows, :].astype(F32)
            saved = moe[rows, :].astype(F32)
            cot_out[b] = (
                cols[:, b : b + 1] * scaled - saved * cols[:, 8 + b : 9 + b]
            ).astype(BF16)
        begin(cot_hop)
        gate_hops[0].arrived()
        begin(gate_hops[1])

    def cotangent_table():
        cot_hop.arrived()
        for h in range(2):
            cot_table[h, 0] = jnp.zeros((8, 128), BF16)

            def pieces(g, h=h):
                return [
                    cot_in[4 * h + b // 2, 32 * g : 32 * (g + 1), b % 2 * 128 : b % 2 * 128 + 128]
                    for b in range(8)
                ]

            def put(g, tiles, h=h):
                cot_table[h, 1 + 32 * g : 33 + 32 * g] = tiles.reshape(32, 8, 128)

            tile_pair(pack_perm, pieces, put)
        gate_hops[1].arrived()
        begin(gate_hops[2])

    def unpack(src, dst, row, half):
        def put(g, b, rows):
            dst[
                row + 32 * g : row + 32 * (g + 1), 1024 * half + 128 * b : 1024 * half + 128 * b + 128
            ] = rows

        row_pair(unpack_perm, lambda g: src[g].reshape(256, 128), put)

    def hidden_inputs(r):
        need(3, 4)
        for h in range(2):
            hops["T", 2 * r + h][2].arrived()
            unpack(t_out.at[2 * r + h], x_rows, 0, h)

        def body(n, carry):
            cols = pl.ds(pl.multiple_of(n * 256, 256), 256)
            x = x_rows[...]
            pre_gate[r, :, cols] = dot(x, wg[:, cols])
            pre_up[r, :, cols] = dot(x, wu[:, cols])
            return carry

        lax.fori_loop(0, 3, body, 0)

        def turned(n, carry):
            cols = pl.ds(pl.multiple_of(n * 256, 256), 256)
            x_t[cols, 128 * r : 128 * (r + 1)] = x_rows[:, cols].T
            return carry

        lax.fori_loop(0, 8, turned, 0)

    def half_back(r, h):
        rows = slice(128 * r, 128 * (r + 1))

        def body(n, carry):
            wide = pl.ds(pl.multiple_of(1024 * h + n * 512, 512), 512)
            total = dot(d_gate[rows, :], wg_t[:, wide]) + dot(d_up[rows, :], wu_t[:, wide])
            back_rows[:, pl.ds(pl.multiple_of(n * 512, 512), 512)] = total.astype(BF16)
            return carry

        lax.fori_loop(0, 2, body, 0)

        hops["T", 2 * r + h][0].left()

        def pieces(g):
            return [
                back_rows[32 * g : 32 * (g + 1), 128 * b : 128 * (b + 1)] for b in range(8)
            ]

        def put(g, tiles):
            t_src[2 * r + h, g] = tiles.reshape(4, 8, 8, 128)

        tile_pair(pack_perm, pieces, put)

    def gate_of(r):
        gates = jnp.concatenate(
            [g_out[z, x][:, 0, :] for z in range(4) for x in range(4)], axis=0
        )
        return gates[:, r : r + 1]

    def slopes(r):
        if r == 0:
            gate_hops[2].arrived()
        for h in range(2):
            hops["C", 2 * r + h][2].arrived()
            unpack(c_out.at[2 * r + h], cot_rows, 128 * r, h)
        gate = gate_of(r)
        rows = slice(128 * r, 128 * (r + 1))

        def body(n, carry):
            cols = pl.ds(pl.multiple_of(n * 256, 256), 256)
            hid_grad = dot(cot_rows[rows, :], wd_t[:, cols])
            p_gate, p_up = pre_gate[r, :, cols], pre_up[r, :, cols]
            sig = jax.nn.sigmoid(p_gate)
            act = p_gate * sig
            hid = act * p_up
            d_hid = gate * hid_grad
            d_gate[rows, cols] = (d_hid * p_up * sig * (1.0 + p_gate * (1.0 - sig))).astype(BF16)
            d_up[rows, cols] = (d_hid * act).astype(BF16)
            hidden[rows, cols] = hid.astype(BF16)
            return carry + jnp.sum(hid * hid_grad, axis=1, keepdims=True)

        total = lax.fori_loop(0, 3, body, jnp.zeros((128, 1), F32))
        slope[...] = jnp.where(iota((128, 128), 1) == r, total, slope[...])
        half_back(r, 0)

    def rest(r):
        half_back(r, 1)
        if r == 2:
            for z in range(4):
                for x in range(4):
                    q_src[z, x, :, 0, :] = slope[32 * z + 8 * x : 32 * z + 8 * x + 8, :]
            begin(slope_hops[0])

    def turn(src, dst):
        def body(n, carry):
            rows = pl.ds(pl.multiple_of(n * 256, 256), 256)
            dst[:, rows] = src[rows, :].T
            return carry

        lax.fori_loop(0, src.shape[0] // 256, body, 0)

    def turn_weight(i):
        if i == 0:
            need(5)
            turn(down_grad, wd_t)
        elif i == 1:
            need(3)
            turn(gate_grad, wg_t)
        else:
            need(4)
            turn(up_grad, wu_t)

    def scale(r):
        rows = slice(128 * r, 128 * (r + 1))
        cot_rows[rows, :] = (gate_of(r) * cot_rows[rows, :].astype(F32)).astype(BF16)

    def weight_grad(i):
        if i >= 8:
            rows = slice(256 * (i - 8), 256 * (i - 7))
            down_grad[rows, :] = dot(hidden[:, rows], cot_rows[...], 0, 0).astype(BF16)
            return
        out, right = ((gate_grad, d_gate), (up_grad, d_up))[i // 4]

        def body(n, carry):
            rows = pl.ds(pl.multiple_of(512 * (i % 4) + n * 256, 256), 256)
            out[rows, :] = dot(x_t[rows, :], right[...]).astype(BF16)
            return carry

        lax.fori_loop(0, 2, body, 0)

    lasts = (86, 98)
    for i, step in enumerate(PLAN):
        kind = step[0]
        if step == "bar":
            pl.semaphore_wait(pltpu.get_barrier_semaphore(), 13)
        elif step == "stat":
            norm_statistics()
        elif step == "cot":
            cotangents()
        elif step == "table":
            cotangent_table()
        elif kind == "A":
            hidden_inputs(int(step[1]))
        elif kind == "B":
            slopes(int(step[1]))
        elif kind == "D":
            rest(int(step[1]))
        elif kind == "M":
            turn_weight(int(step[1]))
        elif kind == "S":
            scale(int(step[1]))
        elif kind == "W":
            weight_grad(int(step[1:]))
        else:
            c, d = int(step[1]), step[2]
            done = hops.setdefault((kind, c), [])
            k = len(done)
            bufs = families[kind]
            if k:
                done[-1].arrived()
            elif kind == "T":
                pack(index_ref, c // 2, table_ref, c % 2, t_src.at[c])
            elif kind == "C":
                pack(index_ref, c // 2, cot_table, c % 2, c_src.at[c])
            n = "TCR".index(kind) * 8 + c
            hop = Hop(
                d, AXIS[d], bufs[k].at[c], bufs[k + 1].at[c],
                (ssem.at[n, k], rsem.at[n, k], lsem.at[n, k]),
            )
            begin(hop)
            done.append(hop)
            if i in (lasts[0], lasts[1]):
                slope_hops[lasts.index(i)].arrived()
                begin(slope_hops[lasts.index(i) + 1])
    for c in range(8):
        hops["R", c][2].arrived()
    slope_hops[2].arrived()
    for hop in every:
        hop.left()


def finish_kernel(
    spot_ref, back_ref, slope_ref, pick_ref, gate_grad, up_grad, down_grad,
    token_ref, gates_ref, gate_out, up_out, down_out, sums, sem,
):
    copies = [
        pltpu.make_async_copy(a, b.at[0], sem.at[i])
        for i, (a, b) in enumerate(
            ((gate_grad, gate_out), (up_grad, up_out), (down_grad, down_out))
        )
    ]
    for copy in copies:
        copy.start()

    def body(i, carry):
        for j in range(8):
            t = i * 8 + j
            for h in range(2):
                one = back_ref[spot_ref[0, t] + 128 * h].astype(F32)
                two = back_ref[spot_ref[1, t] + 128 * h].astype(F32)
                sums[h, t] = (one + two).astype(BF16)
        return carry

    lax.fori_loop(0, 16, body, 0)
    perm = to_rows()
    for h in range(2):

        def put(g, b, rows, h=h):
            token_ref[32 * g : 32 * (g + 1), 1024 * h + 128 * b : 1024 * h + 128 * (b + 1)] = rows

        row_pair(perm, lambda g, h=h: sums[h, 32 * g : 32 * (g + 1)].reshape(256, 128), put)
    slope = slope_ref[:, 0, :].astype(BF16)
    pick = pick_ref[...]
    lane = iota((128, 128), 1)
    lane_f = lane.astype(F32)
    both = jnp.zeros((128, 128), F32)
    for k in range(2):
        one = (pick[:, 2 + k : 3 + k] == lane_f).astype(F32).astype(BF16)
        mine = jnp.where(lane_f == pick[:, 4 + k : 5 + k], dot(one, slope), 0.0)
        both = jnp.where(lane == k, jnp.sum(mine, axis=1, keepdims=True), both)
    gates_ref[...] = both.T[:2].astype(BF16)
    for copy in copies:
        copy.wait()


def struct(shape, dtype=BF16):
    return jax.ShapeDtypeStruct(shape, dtype)


def local(tokens, routes, gates, w_gate, w_up, w_down, moe_out, norm_gain, out_grad):
    pieces = (8, 4, 4, 8, 8, 128)
    lanes = (4, 4, 8, 1, 128)
    deep, flat = (2048, 768), (768, 2048)
    rows, inner = (512, 2048), (512, 768)
    back, slope, spot, pick, gate_grad, up_grad, down_grad = pl.pallas_call(
        mega_kernel,
        out_shape=(
            pltpu.VMEM(pieces, BF16),
            pltpu.VMEM(lanes, F32),
            struct((8, 128), jnp.int32),
            pltpu.VMEM((128, 128), F32),
            pltpu.VMEM(deep, BF16),
            pltpu.VMEM(deep, BF16),
            pltpu.VMEM(flat, BF16),
        ),
        in_specs=[VMEM] * 3 + [ANY] * 6,
        out_specs=(VMEM,) * 7,
        scratch_shapes=[
            pltpu.VMEM((128, 2048), BF16),
            pltpu.VMEM((1024, 256), BF16),
            pltpu.VMEM((1024, 256), BF16),
            pltpu.VMEM((8, 128), jnp.int32),
            pltpu.SMEM((8, 128), jnp.int32),
            pltpu.VMEM(lanes, F32),
            pltpu.VMEM((2, 129, 8, 128), BF16),
            pltpu.VMEM((2, 8, 128), F32),
            pltpu.VMEM(flat, BF16),
            pltpu.VMEM(flat, BF16),
            pltpu.VMEM(deep, BF16),
            *[pltpu.VMEM(pieces, BF16)] * 10,
            *[pltpu.VMEM(lanes, F32)] * 6,
            pltpu.VMEM((8, 2, 8, 128), F32),
            pltpu.VMEM((8, 128, 256), BF16),
            pltpu.VMEM((8, 128, 256), BF16),
            pltpu.VMEM((2, 129, 8, 128), BF16),
            pltpu.VMEM((128, 2048), BF16),
            pltpu.VMEM((2048, 512), BF16),
            pltpu.VMEM(inner, BF16),
            pltpu.VMEM(inner, BF16),
            pltpu.VMEM(inner, BF16),
            pltpu.VMEM((4, 128, 768), F32),
            pltpu.VMEM((4, 128, 768), F32),
            pltpu.VMEM(rows, BF16),
            pltpu.VMEM((128, 1024), BF16),
            pltpu.VMEM((128, 128), F32),
            pltpu.SemaphoreType.DMA((24, 3)),
            pltpu.SemaphoreType.DMA((24, 3)),
            pltpu.SemaphoreType.DMA((24, 3)),
            pltpu.SemaphoreType.DMA((8, 3)),
            pltpu.SemaphoreType.DMA((7,)),
        ],
        compiler_params=pltpu.CompilerParams(
            collective_id=0, has_side_effects=True, vmem_limit_bytes=46 << 20
        ),
        name="exchange",
    )(
        routes.T, gates.T, norm_gain.reshape(1, 256), tokens, moe_out, out_grad,
        w_gate[0], w_up[0], w_down[0],
    )
    token_grad, gates_grad, *grads = pl.pallas_call(
        finish_kernel,
        out_shape=(
            struct((128, 2048)),
            struct((2, 128)),
            struct((1, *deep)),
            struct((1, *deep)),
            struct((1, *flat)),
        ),
        in_specs=[SMEM] + [VMEM] * 6,
        out_specs=(VMEM, VMEM, ANY, ANY, ANY),
        scratch_shapes=[pltpu.VMEM((2, 128, 8, 128), BF16), pltpu.SemaphoreType.DMA((3,))],
        compiler_params=pltpu.CompilerParams(vmem_limit_bytes=8 << 20),
        name="finish",
    )(spot, back.reshape(1024, 8, 128), slope.reshape(128, 1, 128), pick, gate_grad, up_grad, down_grad)
    return (token_grad, gates_grad.T, *grads)


def solution(mesh):
    split = P(("ep", "tp"), None)
    expert = P(("ep", "tp"), None, None)
    in_specs = (split, split, split, expert, expert, expert, P("ep", "tp"), P("tp"), P("ep", "tp"))
    out_specs = (split, split, expert, expert, expert)
    return jax.shard_map(local, mesh=mesh, in_specs=in_specs, out_specs=out_specs, check_vma=False)
```

```python
import jax
import jax.numpy as jnp
from jax import lax
from jax.experimental import pallas as pl
from jax.experimental.pallas import tpu as pltpu
from jax.sharding import PartitionSpec as P

F32 = jnp.float32
BF16 = jnp.bfloat16
MESH = pl.DeviceIdType.MESH
VMEM = pl.BlockSpec(memory_space=pltpu.VMEM)
SMEM = pl.BlockSpec(memory_space=pltpu.SMEM)
ANY = pl.BlockSpec(memory_space=pl.ANY)
SIZE = {"z": 4, "x": 4, "t": 8}
AXIS = {"z": 0, "x": 1, "t": 2}
epsilon = 1e-06

PLAN = (
    "bar", "stat", "T3t", "T2z", "T0t", "T6x", "T1z", "T7z", "T4t", "T5x", "cot", "C0x",
    "C1t", "C5z", "C2t", "T2x", "T0z", "T1t", "C7t", "M0", "T3x", "C3x", "C4t", "M1",
    "C0z", "T5z", "C1x", "C2z", "T0x", "C0t", "T1x", "C3z", "C1z", "C6t", "M2", "T2t",
    "T3z", "T4x", "C5x", "C3t", "C2x", "C4z", "T7t", "C7x", "T5t", "T6z", "A0", "B0",
    "T4z", "A1", "C4x", "D0", "C5t", "R1x", "C6z", "B1", "T6t", "R2z", "R0t", "D1",
    "C7z", "T7x", "A2", "C6x", "R3z", "B2", "R1t", "R4z", "D2", "R5t", "R2x", "A3",
    "R0x", "B3", "R6t", "D3", "R7z", "S3", "R3x", "S0", "R4t", "W0", "R5x", "R2t",
    "R1z", "R6z", "R7x", "W3", "R3t", "W7", "R4x", "S1", "S2", "R0z", "R5z", "W10",
    "W5", "W4", "R6x", "R7t", "W2", "W1", "W9", "W8", "W6",
)


def iota(shape, dim):
    return lax.broadcasted_iota(jnp.int32, shape, dim)


def dot(a, b, a_dim=1, b_dim=0):
    return lax.dot_general(
        a, b, (((a_dim,), (b_dim,)), ((), ())), preferred_element_type=F32
    )


def to_rows():
    i, j = iota((256, 256), 0), iota((256, 256), 1)
    return (((i >> 5) == (j & 7)) & ((i & 31) == (j >> 3))).astype(F32).astype(BF16)


def to_tiles():
    i, j = iota((256, 256), 0), iota((256, 256), 1)
    return (((i >> 3) == (j & 31)) & ((i & 7) == (j >> 5))).astype(F32).astype(BF16)


def to_expert_rows():
    i, j = iota((256, 256), 0), iota((256, 256), 1)
    place = (((i >> 2) & 3) << 3) | (((i >> 4) & 1) << 2) | (i & 3)
    return (j == ((place << 3) | (i >> 5))).astype(F32).astype(BF16)


def from_expert_rows():
    j, i = iota((256, 256), 0), iota((256, 256), 1)
    place = (((i >> 2) & 3) << 3) | (((i >> 4) & 1) << 2) | (i & 3)
    return (j == ((place << 3) | (i >> 5))).astype(F32).astype(BF16)


def to_expert_cols():
    i, j = iota((256, 256), 0), iota((256, 256), 1)
    spot = (((i >> 2) & 3) << 6) | ((i >> 5) << 3) | ((i & 3) << 1) | ((i >> 4) & 1)
    return (j == spot).astype(F32).astype(BF16)


def expert_order():
    i, j = iota((128, 128), 0), iota((128, 128), 1)
    place = ((i >> 5) << 5) | (((i >> 2) & 3) << 3) | (((i >> 4) & 1) << 2) | (i & 3)
    return (j == place).astype(F32).astype(BF16)


def tile_pair(perm, pieces, put):
    for pair in range(2):
        both = jnp.concatenate(
            [jnp.concatenate(pieces(2 * pair + j), axis=0) for j in range(2)], axis=1
        )
        out = dot(perm, both).astype(BF16)
        for j in range(2):
            put(2 * pair + j, out[:, 128 * j : 128 * (j + 1)])


def row_pair(perm, tiles, put):
    for pair in range(2):
        both = jnp.concatenate([tiles(2 * pair + j) for j in range(2)], axis=1)
        out = dot(perm, both).astype(BF16)
        for j in range(2):
            for b in range(8):
                put(2 * pair + j, b, out[32 * b : 32 * (b + 1), 128 * j : 128 * (j + 1)])


def statistics(moe, grad, gain_ref, stat_ref):
    for b in range(8):
        rows = slice(128 * b, 128 * (b + 1))
        saved = moe[rows, :].astype(F32)
        scaled = gain_ref[...] * grad[rows, :].astype(F32)
        for s, prod in enumerate((saved * saved, saved * scaled)):
            part = (prod[:, :128] + prod[:, 128:]).T
            stat_ref[s, b : b + 1, :] = jnp.sum(part, axis=0, keepdims=True)


def routing(routes_ref, gates_ref, index_ref, stat_ref, spot_ref, gate_ref, pick_ref):
    head = jnp.concatenate(
        [routes_ref[...].astype(F32), gates_ref[...], jnp.zeros((4, 128), F32)], axis=0
    )
    cols = head.T
    lane, row = iota((128, 128), 1), iota((128, 128), 0)
    lane_f = lane.astype(F32)
    below = (lane < row).astype(F32).astype(BF16)
    hot = [(cols[:, k : k + 1] == lane_f).astype(F32) for k in range(2)]
    seen = dot(below, (hot[0] + hot[1]).astype(BF16))
    rank = [jnp.sum(hot[k] * seen, axis=1, keepdims=True) for k in range(2)]
    number = (row + 1).astype(F32)
    index = jnp.zeros((128, 128), F32)
    gate = jnp.zeros((128, 128), F32)
    for k in range(2):
        at = lane_f == rank[k]
        one = hot[k].astype(BF16)
        index += dot(jnp.where(at, number, 0.0).astype(BF16), one, 0, 0)
        gate += dot(one, jnp.where(at, cols[:, 2 + k : 3 + k], 0.0).astype(BF16), 0, 0)
    index_ref[...] = jnp.clip(index[:8].astype(jnp.int32), 0, 128)
    stat_ref[2] = index[:8]
    for z in range(4):
        for x in range(4):
            gate_ref[z, x, :, 0, :] = gate[32 * z + 8 * x : 32 * z + 8 * x + 8, :]
    pick = jnp.zeros((128, 128), F32)
    for k in range(2):
        pick = jnp.where(lane == k, rank[k] * 256.0 + cols[:, k : k + 1], pick)
        pick = jnp.where(lane == 2 + k, cols[:, k : k + 1], pick)
        pick = jnp.where(lane == 4 + k, rank[k], pick)
    pick_ref[...] = pick
    spot_ref[...] = pick.T[:8].astype(jnp.int32)


def token_table(perm, tokens, table_ref):
    for h in range(2):
        table_ref[h, 0] = jnp.zeros((8, 128), BF16)

        def pieces(g, h=h):
            return [
                tokens[32 * g : 32 * (g + 1), 1024 * h + 128 * b : 1024 * h + 128 * (b + 1)]
                for b in range(8)
            ]

        def put(g, tiles, h=h):
            table_ref[h, 1 + 32 * g : 33 + 32 * g] = tiles.reshape(32, 8, 128)

        tile_pair(perm, pieces, put)


def coords():
    ep = lax.axis_index("ep")
    return {"z": ep // 4, "x": ep % 4, "t": lax.axis_index("tp")}


def peers(dim, here):
    if dim != "t":
        return [(here + k) % 4 for k in (1, 3, 2)]
    return [
        (here // 2 + dy) % 4 * 2 + (here % 2 + dc) % 2
        for dy, dc in ((1, 0), (3, 0), (1, 1), (3, 1), (2, 0), (2, 1), (0, 1))
    ]


def others():
    me = coords()
    for dim in "zxt":
        for p in peers(dim, me[dim]):
            place = {**me, dim: p}
            yield dim, p, (place["z"] * 4 + place["x"], place["t"])


def greet():
    for _, _, device in others():
        pl.semaphore_signal(
            pltpu.get_barrier_semaphore(), inc=1, device_id=device, device_id_type=MESH
        )


def cut(ref, axis, index):
    return ref.at[(slice(None),) * axis + (index,)]


class Hop:
    def __init__(self, dim, axis, src, dst, sems, whole=False):
        self.dim, self.axis, self.whole, self.gone = dim, axis, whole, False
        self.src, self.dst, (self.ssem, self.rsem, self.lsem) = src, dst, sems

    def piece(self, index):
        return self.src if self.whole else cut(self.src, self.axis, index)

    def start(self):
        mine = coords()[self.dim]
        for dim, p, device in others():
            if dim == self.dim:
                pltpu.make_async_remote_copy(
                    self.piece(p),
                    cut(self.dst, self.axis, mine),
                    self.ssem,
                    self.rsem,
                    device_id=device,
                    device_id_type=MESH,
                ).start()
        pltpu.make_async_copy(self.piece(mine), cut(self.dst, self.axis, mine), self.lsem).start()

    def remote_part(self):
        return cut(self.dst, self.axis, slice(0, SIZE[self.dim] - 1))

    def arrived(self):
        part = self.remote_part()
        pltpu.make_async_copy(part, part, self.rsem).wait()
        one = cut(self.dst, self.axis, 0)
        pltpu.make_async_copy(one, one, self.lsem).wait()

    def left(self):
        if self.gone:
            return
        self.gone = True
        part = self.remote_part()
        pltpu.make_async_copy(part, part, self.ssem).wait()


def pack(index_ref, rank, table_ref, half, dst):
    def body(i, carry):
        for t in range(8):
            dst[i // 4, i % 4, t] = table_ref[half, index_ref[rank, i * 8 + t]]
        return carry

    lax.fori_loop(0, 16, body, 0)


def mega_kernel(
    routes_ref, gates_ref, gain_ref, tokens_any, moe_any, grad_any, wg_any, wu_any, wd_any,
    back_ref, slope_ref, spot_ref, pick_ref, gate_grad, up_grad, down_grad,
    tokens, moe, grad, index_v, index_ref, gate_src, table_ref, stat_ref,
    wg_t, wu_t, wd_t, t_src, t_one, t_two, t_out, c_src, c_one, c_two, c_out, r_one, r_two,
    g_one, g_two, g_out, q_src, q_one, q_two, s_in, cot_parts, index_cols, gate_cols,
    x_rows, x_t, d_gate, d_up, hidden, pre_gate, pre_up, cot_rows, back_rows, slope,
    ssem, rsem, lsem, misc, wsem,
):
    wg, wu = gate_grad, up_grad
    loads = [
        pltpu.make_async_copy(a, b, wsem.at[i])
        for i, (a, b) in enumerate(
            (
                (moe_any, moe), (grad_any, grad), (tokens_any, tokens),
                (wg_any, gate_grad), (wu_any, up_grad), (wd_any, down_grad),
            )
        )
    ]
    loaded = set()

    def need(*which):
        for i in which:
            if i not in loaded:
                loads[i].wait()
                loaded.add(i)

    for load in loads:
        load.start()
    greet()
    slope[...] = jnp.zeros((128, 128), F32)
    routing(routes_ref, gates_ref, index_v, stat_ref, spot_ref, gate_src, pick_ref)
    index_copy = pltpu.make_async_copy(index_v, index_ref, wsem.at[6])
    index_copy.start()
    need(0, 1)
    statistics(moe, grad, gain_ref, stat_ref)
    need(2)
    token_table(to_tiles(), tokens, table_ref)
    index_copy.wait()
    families = {
        "T": (t_src, t_one, t_two, t_out),
        "C": (c_src, c_one, c_two, c_out),
        "R": (t_src, r_one, r_two, back_ref),
    }
    hops = {}
    every = []

    def small(i):
        return tuple(misc.at[i, j] for j in range(3))

    stat_hop = Hop("t", 0, stat_ref, s_in, small(0), whole=True)
    gate_hops = [
        Hop(d, AXIS[d], a, b, small(2 + i))
        for i, (d, a, b) in enumerate(
            (("x", gate_src, g_one), ("t", g_one, g_two), ("z", g_two, g_out))
        )
    ]
    slope_hops = [
        Hop(d, AXIS[d], a, b, small(5 + i))
        for i, (d, a, b) in enumerate(
            (("x", q_src, q_one), ("t", q_one, q_two), ("z", q_two, slope_ref))
        )
    ]

    def begin(hop):
        hop.start()
        every.append(hop)

    def norm_statistics():
        begin(stat_hop)
        begin(gate_hops[0])

    def cotangents():
        stat_hop.arrived()
        total = s_in[0]
        for p in range(1, 8):
            total += s_in[p]
        inv = lax.rsqrt(total[0] / 2048.0 + epsilon)
        cols = jnp.concatenate([inv, inv**3 * total[1] / 2048.0], axis=0).T

        for b in range(8):
            rows = slice(128 * b, 128 * (b + 1))
            scaled = gain_ref[...] * grad[rows, :].astype(F32)
            saved = moe[rows, :].astype(F32)
            cot_parts[b] = (
                cols[:, b : b + 1] * scaled - saved * cols[:, 8 + b : 9 + b]
            ).astype(BF16)
        index_cols[...] = jnp.concatenate(
            [s_in[b, 2] for b in range(8)] + [jnp.zeros((64, 128), F32)], axis=0
        ).T
        gate_hops[0].arrived()
        begin(gate_hops[1])

    def pack_cotangents(c, dst):
        rank, half = c // 2, c % 2
        number = (iota((128, 128), 1) + 1).astype(F32)
        parts = []
        for b in range(4 * half, 4 * half + 4):
            index = index_cols[:, 8 * b + rank : 8 * b + rank + 1]
            chosen = (index == number).astype(F32).astype(BF16)
            parts.append(dot(chosen, cot_parts[b]).astype(BF16))

        def pieces(g):
            return [
                part[32 * g : 32 * (g + 1), 128 * b : 128 * (b + 1)]
                for part in parts
                for b in range(2)
            ]

        def put(g, tiles):
            dst[g] = tiles.reshape(4, 8, 8, 128)

        tile_pair(to_tiles(), pieces, put)

    def unpack(src, dst, row, half):
        def put(g, b, rows):
            dst[
                row + 32 * g : row + 32 * (g + 1), 1024 * half + 128 * b : 1024 * half + 128 * b + 128
            ] = rows

        row_pair(to_expert_rows(), lambda g: src[g].reshape(256, 128), put)

    def unpack_cotangents(src, row, half):
        perm = to_expert_cols()
        for pair in range(2):
            both = jnp.concatenate([src[2 * pair + j].reshape(256, 128) for j in range(2)], axis=1)
            out = dot(perm, both).astype(BF16)
            for j in range(2):
                at = row + 32 * (2 * pair + j) + 16 * half
                for b in range(16):
                    cot_rows[at : at + 16, 128 * b : 128 * (b + 1)] = out[
                        16 * b : 16 * (b + 1), 128 * j : 128 * (j + 1)
                    ]

    def hidden_inputs(r):
        need(3, 4)
        for h in range(2):
            hops["T", 2 * r + h][2].arrived()
            unpack(t_out.at[2 * r + h], x_rows, 0, h)

        def body(n, carry):
            cols = pl.ds(pl.multiple_of(n * 256, 256), 256)
            x = x_rows[...]
            pre_gate[r, :, cols] = dot(x, wg[:, cols])
            pre_up[r, :, cols] = dot(x, wu[:, cols])
            return carry

        lax.fori_loop(0, 3, body, 0)

        def turned(n, carry):
            cols = pl.ds(pl.multiple_of(n * 256, 256), 256)
            x_t[cols, 128 * r : 128 * (r + 1)] = x_rows[:, cols].T
            return carry

        lax.fori_loop(0, 8, turned, 0)

    def half_back(r, h):
        rows = slice(128 * r, 128 * (r + 1))

        def body(n, carry):
            wide = pl.ds(pl.multiple_of(1024 * h + n * 512, 512), 512)
            total = dot(d_gate[rows, :], wg_t[:, wide]) + dot(d_up[rows, :], wu_t[:, wide])
            back_rows[:, pl.ds(pl.multiple_of(n * 512, 512), 512)] = total.astype(BF16)
            return carry

        lax.fori_loop(0, 2, body, 0)

        hops["T", 2 * r + h][0].left()

        def pieces(g):
            return [
                back_rows[32 * g : 32 * (g + 1), 128 * b : 128 * (b + 1)] for b in range(8)
            ]

        def put(g, tiles):
            t_src[2 * r + h, g] = tiles.reshape(4, 8, 8, 128)

        tile_pair(from_expert_rows(), pieces, put)

    def gate_of(r):
        return gate_cols[:, r : r + 1]

    def slopes(r):
        if r == 0:
            gate_hops[2].arrived()
            gates = jnp.concatenate(
                [g_out[z, x][:, 0, :] for z in range(4) for x in range(4)], axis=0
            )
            gate_cols[...] = dot(expert_order(), gates.astype(BF16))
        for h in range(2):
            hops["C", 2 * r + h][2].arrived()
            unpack_cotangents(c_out.at[2 * r + h], 128 * r, h)
        gate = gate_of(r)
        rows = slice(128 * r, 128 * (r + 1))

        def body(n, carry):
            cols = pl.ds(pl.multiple_of(n * 256, 256), 256)
            hid_grad = dot(cot_rows[rows, :], wd_t[:, cols])
            p_gate, p_up = pre_gate[r, :, cols], pre_up[r, :, cols]
            sig = jax.nn.sigmoid(p_gate)
            act = p_gate * sig
            hid = act * p_up
            d_hid = gate * hid_grad
            d_gate[rows, cols] = (d_hid * p_up * sig * (1.0 + p_gate * (1.0 - sig))).astype(BF16)
            d_up[rows, cols] = (d_hid * act).astype(BF16)
            hidden[rows, cols] = hid.astype(BF16)
            return carry + jnp.sum(hid * hid_grad, axis=1, keepdims=True)

        total = lax.fori_loop(0, 3, body, jnp.zeros((128, 1), F32))
        slope[...] = jnp.where(iota((128, 128), 1) == r, total, slope[...])
        half_back(r, 0)

    def rest(r):
        half_back(r, 1)
        if r == 3:
            slope[...] = dot(expert_order(), slope[...].astype(BF16), 0, 0)
            for z in range(4):
                for x in range(4):
                    q_src[z, x, :, 0, :] = slope[32 * z + 8 * x : 32 * z + 8 * x + 8, :]
            begin(slope_hops[0])

    def turn(src, dst):
        def body(n, carry):
            rows = pl.ds(pl.multiple_of(n * 256, 256), 256)
            dst[:, rows] = src[rows, :].T
            return carry

        lax.fori_loop(0, src.shape[0] // 256, body, 0)

    def turn_weight(i):
        if i == 0:
            need(5)
            turn(down_grad, wd_t)
        elif i == 1:
            need(3)
            turn(gate_grad, wg_t)
        else:
            need(4)
            turn(up_grad, wu_t)

    def scale(r):
        rows = slice(128 * r, 128 * (r + 1))
        cot_rows[rows, :] = (gate_of(r) * cot_rows[rows, :].astype(F32)).astype(BF16)

    def weight_grad(i):
        if i >= 8:
            rows = slice(256 * (i - 8), 256 * (i - 7))
            down_grad[rows, :] = dot(hidden[:, rows], cot_rows[...], 0, 0).astype(BF16)
            return
        out, right = ((gate_grad, d_gate), (up_grad, d_up))[i // 4]

        def body(n, carry):
            rows = pl.ds(pl.multiple_of(512 * (i % 4) + n * 256, 256), 256)
            out[rows, :] = dot(x_t[rows, :], right[...]).astype(BF16)
            return carry

        lax.fori_loop(0, 2, body, 0)

    early = [step for step in PLAN if step[0] == "T"][:3]
    for step in early:
        c = int(step[1])
        pack(index_ref, c // 2, table_ref, c % 2, t_src.at[c])
    lasts = (85, 94)
    for i, step in enumerate(PLAN):
        kind = step[0]
        if step == "bar":
            pl.semaphore_wait(pltpu.get_barrier_semaphore(), 13)
        elif step == "stat":
            norm_statistics()
        elif step == "cot":
            cotangents()
        elif kind == "A":
            hidden_inputs(int(step[1]))
        elif kind == "B":
            slopes(int(step[1]))
        elif kind == "D":
            rest(int(step[1]))
        elif kind == "M":
            turn_weight(int(step[1]))
        elif kind == "S":
            scale(int(step[1]))
        elif kind == "W":
            weight_grad(int(step[1:]))
        else:
            c, d = int(step[1]), step[2]
            done = hops.setdefault((kind, c), [])
            k = len(done)
            bufs = families[kind]
            if k:
                done[-1].arrived()
            elif kind == "T" and step not in early:
                pack(index_ref, c // 2, table_ref, c % 2, t_src.at[c])
            elif kind == "C":
                pack_cotangents(c, c_src.at[c])
            n = "TCR".index(kind) * 8 + c
            hop = Hop(
                d, AXIS[d], bufs[k].at[c], bufs[k + 1].at[c],
                (ssem.at[n, k], rsem.at[n, k], lsem.at[n, k]),
            )
            begin(hop)
            done.append(hop)
            if i == 21:
                gate_hops[1].arrived()
                begin(gate_hops[2])
            if i in (lasts[0], lasts[1]):
                slope_hops[lasts.index(i)].arrived()
                begin(slope_hops[lasts.index(i) + 1])
    for c in range(8):
        hops["R", c][2].arrived()
    slope_hops[2].arrived()
    for hop in every:
        hop.left()


def finish_kernel(
    spot_any, back_ref, slope_ref, pick_ref, gate_grad, up_grad, down_grad,
    token_ref, gates_ref, gate_out, up_out, down_out, spot_ref, sums, sem,
):
    copies = [
        pltpu.make_async_copy(a, b.at[0], sem.at[i])
        for i, (a, b) in enumerate(
            ((gate_grad, gate_out), (up_grad, up_out), (down_grad, down_out))
        )
    ]
    spots = pltpu.make_async_copy(spot_any, spot_ref, sem.at[3])
    spots.start()
    for copy in copies:
        copy.start()
    spots.wait()

    def body(i, carry):
        for j in range(16):
            t = i * 16 + j
            for h in range(2):
                one = back_ref[spot_ref[0, t] + 128 * h].astype(F32)
                two = back_ref[spot_ref[1, t] + 128 * h].astype(F32)
                sums[h, t] = (one + two).astype(BF16)
        return carry

    lax.fori_loop(0, 8, body, 0)
    perm = to_rows()
    for h in range(2):

        def put(g, b, rows, h=h):
            token_ref[32 * g : 32 * (g + 1), 1024 * h + 128 * b : 1024 * h + 128 * (b + 1)] = rows

        row_pair(perm, lambda g, h=h: sums[h, 32 * g : 32 * (g + 1)].reshape(256, 128), put)
    slope = slope_ref[:, 0, :].astype(BF16)
    pick = pick_ref[...]
    lane = iota((128, 128), 1)
    lane_f = lane.astype(F32)
    both = jnp.zeros((128, 128), F32)
    for k in range(2):
        one = (pick[:, 2 + k : 3 + k] == lane_f).astype(F32).astype(BF16)
        mine = jnp.where(lane_f == pick[:, 4 + k : 5 + k], dot(one, slope), 0.0)
        both = jnp.where(lane == k, jnp.sum(mine, axis=1, keepdims=True), both)
    gates_ref[...] = both.T[:2].astype(BF16)
    for copy in copies:
        copy.wait()


def struct(shape, dtype=BF16):
    return jax.ShapeDtypeStruct(shape, dtype)


def local(tokens, routes, gates, w_gate, w_up, w_down, moe_out, norm_gain, out_grad):
    pieces = (8, 4, 4, 8, 8, 128)
    lanes = (4, 4, 8, 1, 128)
    deep, flat = (2048, 768), (768, 2048)
    rows, inner = (512, 2048), (512, 768)
    back, slope, spot, pick, gate_grad, up_grad, down_grad = pl.pallas_call(
        mega_kernel,
        out_shape=(
            pltpu.VMEM(pieces, BF16),
            pltpu.VMEM(lanes, F32),
            pltpu.VMEM((8, 128), jnp.int32),
            pltpu.VMEM((128, 128), F32),
            pltpu.VMEM(deep, BF16),
            pltpu.VMEM(deep, BF16),
            pltpu.VMEM(flat, BF16),
        ),
        in_specs=[VMEM] * 3 + [ANY] * 6,
        out_specs=(VMEM,) * 7,
        scratch_shapes=[
            pltpu.VMEM((128, 2048), BF16),
            pltpu.VMEM((1024, 256), BF16),
            pltpu.VMEM((1024, 256), BF16),
            pltpu.VMEM((8, 128), jnp.int32),
            pltpu.SMEM((8, 128), jnp.int32),
            pltpu.VMEM(lanes, F32),
            pltpu.VMEM((2, 129, 8, 128), BF16),
            pltpu.VMEM((3, 8, 128), F32),
            pltpu.VMEM(flat, BF16),
            pltpu.VMEM(flat, BF16),
            pltpu.VMEM(deep, BF16),
            *[pltpu.VMEM(pieces, BF16)] * 10,
            *[pltpu.VMEM(lanes, F32)] * 6,
            pltpu.VMEM((8, 3, 8, 128), F32),
            pltpu.VMEM((8, 128, 256), BF16),
            pltpu.VMEM((128, 128), F32),
            pltpu.VMEM((128, 128), F32),
            pltpu.VMEM((128, 2048), BF16),
            pltpu.VMEM((2048, 512), BF16),
            pltpu.VMEM(inner, BF16),
            pltpu.VMEM(inner, BF16),
            pltpu.VMEM(inner, BF16),
            pltpu.VMEM((4, 128, 768), F32),
            pltpu.VMEM((4, 128, 768), F32),
            pltpu.VMEM(rows, BF16),
            pltpu.VMEM((128, 1024), BF16),
            pltpu.VMEM((128, 128), F32),
            pltpu.SemaphoreType.DMA((24, 3)),
            pltpu.SemaphoreType.DMA((24, 3)),
            pltpu.SemaphoreType.DMA((24, 3)),
            pltpu.SemaphoreType.DMA((8, 3)),
            pltpu.SemaphoreType.DMA((7,)),
        ],
        compiler_params=pltpu.CompilerParams(
            collective_id=0, has_side_effects=True, vmem_limit_bytes=46 << 20
        ),
        name="exchange",
    )(
        routes.T, gates.T, norm_gain.reshape(1, 256), tokens, moe_out, out_grad,
        w_gate[0], w_up[0], w_down[0],
    )
    token_grad, gates_grad, *grads = pl.pallas_call(
        finish_kernel,
        out_shape=(
            struct((128, 2048)),
            struct((2, 128)),
            struct((1, *deep)),
            struct((1, *deep)),
            struct((1, *flat)),
        ),
        in_specs=[VMEM] * 7,
        out_specs=(VMEM, VMEM, ANY, ANY, ANY),
        scratch_shapes=[
            pltpu.SMEM((8, 128), jnp.int32),
            pltpu.VMEM((2, 128, 8, 128), BF16),
            pltpu.SemaphoreType.DMA((4,)),
        ],
        compiler_params=pltpu.CompilerParams(vmem_limit_bytes=8 << 20),
        name="finish",
    )(spot, back.reshape(1024, 8, 128), slope.reshape(128, 1, 128), pick, gate_grad, up_grad, down_grad)
    return (token_grad, gates_grad.T, *grads)


def solution(mesh):
    split = P(("ep", "tp"), None)
    expert = P(("ep", "tp"), None, None)
    in_specs = (split, split, split, expert, expert, expert, P("ep", "tp"), P("tp"), P("ep", "tp"))
    out_specs = (split, split, expert, expert, expert)
    return jax.shard_map(local, mesh=mesh, in_specs=in_specs, out_specs=out_specs, check_vma=False)
```

```python
import jax
import jax.numpy as jnp
from jax import lax
from jax.experimental import pallas as pl
from jax.experimental.pallas import tpu as pltpu
from jax.sharding import PartitionSpec as P

F32 = jnp.float32
BF16 = jnp.bfloat16
MESH = pl.DeviceIdType.MESH
VMEM = pl.BlockSpec(memory_space=pltpu.VMEM)
SMEM = pl.BlockSpec(memory_space=pltpu.SMEM)
ANY = pl.BlockSpec(memory_space=pl.ANY)
SIZE = {"z": 4, "x": 4, "t": 8}
AXIS = {"z": 0, "x": 1, "t": 2}
epsilon = 1e-06

PLAN = (
    "bar", "stat", "T1x", "T0z", "T3t", "T7z", "T6x", "T2z", "T4t", "T5x", "T1t", "cot",
    "C6z", "C5t", "C4x", "C7z", "C2t", "T4x", "C1t", "T5z", "T7x", "M1", "C4t", "C0x",
    "C6t", "C5z", "T6z", "C7x", "T4z", "T5t", "M0", "C1x", "C4z", "C0z", "M2", "C5x",
    "T0x", "T7t", "C6x", "C3z", "T1z", "C2x", "T6t", "C7t", "T2t", "A2", "B2", "D2",
    "R5z1", "T0t", "T3x", "C1z", "A3", "S2", "C3x", "C0t", "B3", "R6z0", "D3", "R7t0",
    "R7x1", "R6t1", "T3z", "T2x", "R4z1", "C2z", "R4x0", "A0", "R6t0", "R5x0", "C3t", "B0",
    "R0z0", "R0t1", "R7t1", "R6x1", "D0", "R1z1", "R1z0", "R4t1", "R6x0", "A1", "R5z0", "R7x0",
    "R4t0", "R5x1", "B1", "R2x0", "R2t1", "R6z1", "D1", "S1", "R3x0", "R3z1", "R0t0", "W6",
    "R0x1", "R7z1", "W5", "R7z0", "R1t1", "R4x1", "W1", "R2t0", "S0", "R2z1", "R1x0", "R3t0",
    "W2", "R3x1", "R4z0", "R5t0", "R0x0", "W3", "R5t1", "R0z1", "R2z0", "R1x1", "R1t0", "R2x1",
    "S3", "R3z0", "R3t1", "W9", "W7", "W4", "W10", "W0", "W8",
)


def iota(shape, dim):
    return lax.broadcasted_iota(jnp.int32, shape, dim)


def dot(a, b, a_dim=1, b_dim=0):
    return lax.dot_general(
        a, b, (((a_dim,), (b_dim,)), ((), ())), preferred_element_type=F32
    )


def to_rows():
    i, j = iota((256, 256), 0), iota((256, 256), 1)
    return (((i >> 5) == (j & 7)) & ((i & 31) == (j >> 3))).astype(F32).astype(BF16)


def to_tiles():
    i, j = iota((256, 256), 0), iota((256, 256), 1)
    return (((i >> 3) == (j & 31)) & ((i & 7) == (j >> 5))).astype(F32).astype(BF16)


def to_expert_rows():
    i, j = iota((256, 256), 0), iota((256, 256), 1)
    place = (((i >> 2) & 3) << 3) | (((i >> 4) & 1) << 2) | (i & 3)
    return (j == ((place << 3) | (i >> 5))).astype(F32).astype(BF16)


def from_expert_rows():
    j, i = iota((256, 256), 0), iota((256, 256), 1)
    place = (((i >> 2) & 3) << 3) | (((i >> 4) & 1) << 2) | (i & 3)
    return (j == ((place << 3) | (i >> 5))).astype(F32).astype(BF16)


def to_expert_cols():
    i, j = iota((256, 256), 0), iota((256, 256), 1)
    spot = (((i >> 2) & 3) << 6) | ((i >> 5) << 3) | ((i & 3) << 1) | ((i >> 4) & 1)
    return (j == spot).astype(F32).astype(BF16)


def expert_order():
    i, j = iota((128, 128), 0), iota((128, 128), 1)
    place = ((i >> 5) << 5) | (((i >> 2) & 3) << 3) | (((i >> 4) & 1) << 2) | (i & 3)
    return (j == place).astype(F32).astype(BF16)


def tile_pair(perm, pieces, put):
    for pair in range(2):
        both = jnp.concatenate(
            [jnp.concatenate(pieces(2 * pair + j), axis=0) for j in range(2)], axis=1
        )
        out = dot(perm, both).astype(BF16)
        for j in range(2):
            put(2 * pair + j, out[:, 128 * j : 128 * (j + 1)])


def row_pair(perm, tiles, put):
    for pair in range(2):
        both = jnp.concatenate([tiles(2 * pair + j) for j in range(2)], axis=1)
        out = dot(perm, both).astype(BF16)
        for j in range(2):
            for b in range(8):
                put(2 * pair + j, b, out[32 * b : 32 * (b + 1), 128 * j : 128 * (j + 1)])


def statistics(moe, grad, gain_ref, stat_ref):
    for b in range(8):
        rows = slice(128 * b, 128 * (b + 1))
        saved = moe[rows, :].astype(F32)
        scaled = gain_ref[...] * grad[rows, :].astype(F32)
        for s, prod in enumerate((saved * saved, saved * scaled)):
            part = (prod[:, :128] + prod[:, 128:]).T
            stat_ref[s, b : b + 1, :] = jnp.sum(part, axis=0, keepdims=True)


def routing(routes_ref, gates_ref, index_ref, stat_ref, spot_ref, gate_ref, pick_ref):
    head = jnp.concatenate(
        [routes_ref[...].astype(F32), gates_ref[...], jnp.zeros((4, 128), F32)], axis=0
    )
    cols = head.T
    lane, row = iota((128, 128), 1), iota((128, 128), 0)
    lane_f = lane.astype(F32)
    below = (lane < row).astype(F32).astype(BF16)
    hot = [(cols[:, k : k + 1] == lane_f).astype(F32) for k in range(2)]
    seen = dot(below, (hot[0] + hot[1]).astype(BF16))
    rank = [jnp.sum(hot[k] * seen, axis=1, keepdims=True) for k in range(2)]
    number = (row + 1).astype(F32)
    index = jnp.zeros((128, 128), F32)
    gate = jnp.zeros((128, 128), F32)
    for k in range(2):
        at = lane_f == rank[k]
        one = hot[k].astype(BF16)
        index += dot(jnp.where(at, number, 0.0).astype(BF16), one, 0, 0)
        gate += dot(one, jnp.where(at, cols[:, 2 + k : 3 + k], 0.0).astype(BF16), 0, 0)
    index_ref[...] = jnp.clip(index[:8].astype(jnp.int32), 0, 128)
    stat_ref[2] = index[:8]
    for z in range(4):
        for x in range(4):
            gate_ref[z, x, :, 0, :] = gate[32 * z + 8 * x : 32 * z + 8 * x + 8, :]
    pick = jnp.zeros((128, 128), F32)
    for k in range(2):
        pick = jnp.where(lane == k, rank[k] * 256.0 + cols[:, k : k + 1], pick)
        pick = jnp.where(lane == 2 + k, cols[:, k : k + 1], pick)
        pick = jnp.where(lane == 4 + k, rank[k], pick)
    pick_ref[...] = pick
    spot_ref[...] = pick.T[:8].astype(jnp.int32)


def token_table(perm, tokens, table_ref):
    for h in range(2):
        table_ref[h, 0] = jnp.zeros((8, 128), BF16)

        def pieces(g, h=h):
            return [
                tokens[32 * g : 32 * (g + 1), 1024 * h + 128 * b : 1024 * h + 128 * (b + 1)]
                for b in range(8)
            ]

        def put(g, tiles, h=h):
            table_ref[h, 1 + 32 * g : 33 + 32 * g] = tiles.reshape(32, 8, 128)

        tile_pair(perm, pieces, put)


def coords():
    ep = lax.axis_index("ep")
    return {"z": ep // 4, "x": ep % 4, "t": lax.axis_index("tp")}


def peers(dim, here):
    if dim != "t":
        return [(here + k) % 4 for k in (2, 1, 3)]
    return [
        (here // 2 + dy) % 4 * 2 + (here % 2 + dc) % 2
        for dy, dc in ((2, 0), (2, 1), (1, 0), (3, 0), (1, 1), (3, 1), (0, 1))
    ]


def others():
    me = coords()
    for dim in "zxt":
        for p in peers(dim, me[dim]):
            place = {**me, dim: p}
            yield dim, p, (place["z"] * 4 + place["x"], place["t"])


def greet():
    for _, _, device in others():
        pl.semaphore_signal(
            pltpu.get_barrier_semaphore(), inc=1, device_id=device, device_id_type=MESH
        )


def cut(ref, axis, index):
    return ref.at[(slice(None),) * axis + (index,)]


class Hop:
    def __init__(self, dim, axis, src, dst, sems, whole=False):
        self.dim, self.axis, self.whole, self.gone = dim, axis, whole, False
        self.src, self.dst, (self.ssem, self.rsem, self.lsem) = src, dst, sems

    def piece(self, index):
        return self.src if self.whole else cut(self.src, self.axis, index)

    def start(self):
        mine = coords()[self.dim]
        for dim, p, device in others():
            if dim == self.dim:
                pltpu.make_async_remote_copy(
                    self.piece(p),
                    cut(self.dst, self.axis, mine),
                    self.ssem,
                    self.rsem,
                    device_id=device,
                    device_id_type=MESH,
                ).start()
        pltpu.make_async_copy(self.piece(mine), cut(self.dst, self.axis, mine), self.lsem).start()

    def remote_part(self):
        return cut(self.dst, self.axis, slice(0, SIZE[self.dim] - 1))

    def arrived(self):
        part = self.remote_part()
        pltpu.make_async_copy(part, part, self.rsem).wait()
        one = cut(self.dst, self.axis, 0)
        pltpu.make_async_copy(one, one, self.lsem).wait()

    def left(self):
        if self.gone:
            return
        self.gone = True
        part = self.remote_part()
        pltpu.make_async_copy(part, part, self.ssem).wait()


class PartHop(Hop):
    def __init__(self, dim, part, src, dst, sems):
        core = lax.axis_index("tp") % 2
        kind = core if part == 0 else 1 - core
        self.cross = dim == "t" and part == 1
        self.far = dst.at[:, :, :, 1 - kind]
        src, dst = src.at[:, :, :, kind], dst.at[:, :, :, kind]
        super().__init__(dim, AXIS[dim], src, dst, sems)

    def start(self):
        if self.dim != "t":
            super().start()
            return
        me = coords()
        mine, core = me["t"] // 2, me["t"] % 2
        for k in (2, 1, 3, 0) if self.cross else (2, 1, 3):
            p = (mine + k) % 4
            place = 2 * p + (1 - core if self.cross else core)
            pltpu.make_async_remote_copy(
                cut(self.src, 2, p),
                cut(self.far if self.cross else self.dst, 2, mine),
                self.ssem,
                self.rsem,
                device_id=(me["z"] * 4 + me["x"], place),
                device_id_type=MESH,
            ).start()
        if not self.cross:
            pltpu.make_async_copy(cut(self.src, 2, mine), cut(self.dst, 2, mine), self.lsem).start()

    def remote_part(self):
        return self.dst if self.cross else cut(self.dst, self.axis, slice(0, 3))

    def arrived(self):
        if self.cross:
            pltpu.make_async_copy(self.dst, self.dst, self.rsem).wait()
        else:
            super().arrived()


def pack(index_ref, rank, table_ref, half, dst):
    def body(i, carry):
        for t in range(8):
            dst[i // 4, i % 4, t] = table_ref[half, index_ref[rank, i * 8 + t]]
        return carry

    lax.fori_loop(0, 16, body, 0)


def mega_kernel(
    routes_ref, gates_ref, gain_ref, tokens_any, moe_any, grad_any, wg_any, wu_any, wd_any,
    back_ref, slope_ref, spot_ref, pick_ref, gate_grad, up_grad, down_grad,
    tokens, moe, grad, index_v, index_ref, gate_src, table_ref, stat_ref,
    wg_t, wu_t, wd_t, t_src, t_one, t_two, t_out, c_src, c_one, c_two, c_out, r_src, r_one, r_two,
    g_one, g_two, g_out, q_src, q_one, q_two, s_in, cot_parts, index_cols, gate_cols,
    x_rows, x_t, d_gate, d_up, hidden, pre_gate, pre_up, cot_rows, back_rows, slope,
    ssem, rsem, lsem, misc, wsem,
):
    wg, wu = gate_grad, up_grad
    loads = [
        pltpu.make_async_copy(a, b, wsem.at[i])
        for i, (a, b) in enumerate(
            (
                (moe_any, moe), (grad_any, grad), (tokens_any, tokens),
                (wg_any, gate_grad), (wu_any, up_grad), (wd_any, down_grad),
            )
        )
    ]
    loaded = set()

    def need(*which):
        for i in which:
            if i not in loaded:
                loads[i].wait()
                loaded.add(i)

    for load in loads:
        load.start()
    greet()
    slope[...] = jnp.zeros((128, 128), F32)
    routing(routes_ref, gates_ref, index_v, stat_ref, spot_ref, gate_src, pick_ref)
    index_copy = pltpu.make_async_copy(index_v, index_ref, wsem.at[6])
    index_copy.start()
    need(0, 1)
    statistics(moe, grad, gain_ref, stat_ref)
    need(2)
    token_table(to_tiles(), tokens, table_ref)
    index_copy.wait()
    families = {
        "T": (t_src, t_one, t_two, t_out),
        "C": (c_src, c_one, c_two, c_out),
        "R": (r_src, r_one, r_two, back_ref),
    }
    hops = {}
    every = []

    def small(i):
        return tuple(misc.at[i, j] for j in range(3))

    stat_hop = Hop("t", 0, stat_ref, s_in, small(0), whole=True)
    gate_hops = [
        Hop(d, AXIS[d], a, b, small(2 + i))
        for i, (d, a, b) in enumerate(
            (("x", gate_src, g_one), ("t", g_one, g_two), ("z", g_two, g_out))
        )
    ]
    slope_hops = [
        Hop(d, AXIS[d], a, b, small(5 + i))
        for i, (d, a, b) in enumerate(
            (("x", q_src, q_one), ("t", q_one, q_two), ("z", q_two, slope_ref))
        )
    ]

    def begin(hop):
        hop.start()
        every.append(hop)

    def norm_statistics():
        begin(stat_hop)
        begin(gate_hops[0])

    def cotangents():
        stat_hop.arrived()
        total = s_in[0]
        for p in range(1, 8):
            total += s_in[p]
        inv = lax.rsqrt(total[0] / 2048.0 + epsilon)
        cols = jnp.concatenate([inv, inv**3 * total[1] / 2048.0], axis=0).T

        for b in range(8):
            rows = slice(128 * b, 128 * (b + 1))
            scaled = gain_ref[...] * grad[rows, :].astype(F32)
            saved = moe[rows, :].astype(F32)
            cot_parts[b] = (
                cols[:, b : b + 1] * scaled - saved * cols[:, 8 + b : 9 + b]
            ).astype(BF16)
        index_cols[...] = jnp.concatenate(
            [s_in[b, 2] for b in range(8)] + [jnp.zeros((64, 128), F32)], axis=0
        ).T
        gate_hops[0].arrived()
        begin(gate_hops[1])

    def pack_cotangents(c, dst):
        rank, half = c // 2, c % 2
        number = (iota((128, 128), 1) + 1).astype(F32)
        parts = []
        for b in range(4 * half, 4 * half + 4):
            index = index_cols[:, 8 * b + rank : 8 * b + rank + 1]
            chosen = (index == number).astype(F32).astype(BF16)
            parts.append(dot(chosen, cot_parts[b]).astype(BF16))

        def pieces(g):
            return [
                part[32 * g : 32 * (g + 1), 128 * b : 128 * (b + 1)]
                for part in parts
                for b in range(2)
            ]

        def put(g, tiles):
            dst[g] = tiles.reshape(4, 8, 8, 128)

        tile_pair(to_tiles(), pieces, put)

    def unpack(src, dst, row, half):
        def put(g, b, rows):
            dst[
                row + 32 * g : row + 32 * (g + 1), 1024 * half + 128 * b : 1024 * half + 128 * b + 128
            ] = rows

        row_pair(to_expert_rows(), lambda g: src[g].reshape(256, 128), put)

    def unpack_cotangents(src, row, half):
        perm = to_expert_cols()
        for pair in range(2):
            both = jnp.concatenate([src[2 * pair + j].reshape(256, 128) for j in range(2)], axis=1)
            out = dot(perm, both).astype(BF16)
            for j in range(2):
                at = row + 32 * (2 * pair + j) + 16 * half
                for b in range(16):
                    cot_rows[at : at + 16, 128 * b : 128 * (b + 1)] = out[
                        16 * b : 16 * (b + 1), 128 * j : 128 * (j + 1)
                    ]

    def hidden_inputs(r):
        need(3, 4)
        for h in range(2):
            hops["T", 2 * r + h][2].arrived()
            unpack(t_out.at[2 * r + h], x_rows, 0, h)

        def body(n, carry):
            cols = pl.ds(pl.multiple_of(n * 256, 256), 256)
            x = x_rows[...]
            pre_gate[r, :, cols] = dot(x, wg[:, cols])
            pre_up[r, :, cols] = dot(x, wu[:, cols])
            return carry

        lax.fori_loop(0, 3, body, 0)

        def turned(n, carry):
            cols = pl.ds(pl.multiple_of(n * 256, 256), 256)
            x_t[cols, 128 * r : 128 * (r + 1)] = x_rows[:, cols].T
            return carry

        lax.fori_loop(0, 8, turned, 0)

    def half_back(r, h):
        rows = slice(128 * r, 128 * (r + 1))

        def body(n, carry):
            wide = pl.ds(pl.multiple_of(1024 * h + n * 512, 512), 512)
            total = dot(d_gate[rows, :], wg_t[:, wide]) + dot(d_up[rows, :], wu_t[:, wide])
            back_rows[:, pl.ds(pl.multiple_of(n * 512, 512), 512)] = total.astype(BF16)
            return carry

        lax.fori_loop(0, 2, body, 0)

        def pieces(g):
            return [
                back_rows[32 * g : 32 * (g + 1), 128 * b : 128 * (b + 1)] for b in range(8)
            ]

        def put(g, tiles):
            r_src[2 * r + h, g] = tiles.reshape(4, 4, 2, 8, 128)

        tile_pair(from_expert_rows(), pieces, put)

    def gate_of(r):
        return gate_cols[:, r : r + 1]

    def slopes(r):
        if r == 2:
            gate_hops[2].arrived()
            gates = jnp.concatenate(
                [g_out[z, x][:, 0, :] for z in range(4) for x in range(4)], axis=0
            )
            gate_cols[...] = dot(expert_order(), gates.astype(BF16))
        for h in range(2):
            hops["C", 2 * r + h][2].arrived()
            unpack_cotangents(c_out.at[2 * r + h], 128 * r, h)
        gate = gate_of(r)
        rows = slice(128 * r, 128 * (r + 1))

        def body(n, carry):
            cols = pl.ds(pl.multiple_of(n * 256, 256), 256)
            hid_grad = dot(cot_rows[rows, :], wd_t[:, cols])
            p_gate, p_up = pre_gate[r, :, cols], pre_up[r, :, cols]
            sig = jax.nn.sigmoid(p_gate)
            act = p_gate * sig
            hid = act * p_up
            d_hid = gate * hid_grad
            d_gate[rows, cols] = (d_hid * p_up * sig * (1.0 + p_gate * (1.0 - sig))).astype(BF16)
            d_up[rows, cols] = (d_hid * act).astype(BF16)
            hidden[rows, cols] = hid.astype(BF16)
            return carry + jnp.sum(hid * hid_grad, axis=1, keepdims=True)

        total = lax.fori_loop(0, 3, body, jnp.zeros((128, 1), F32))
        slope[...] = jnp.where(iota((128, 128), 1) == r, total, slope[...])
        half_back(r, 0)

    def rest(r):
        half_back(r, 1)
        if r == 1:
            slope[...] = dot(expert_order(), slope[...].astype(BF16), 0, 0)
            for z in range(4):
                for x in range(4):
                    q_src[z, x, :, 0, :] = slope[32 * z + 8 * x : 32 * z + 8 * x + 8, :]
            begin(slope_hops[0])

    def turn(src, dst):
        def body(n, carry):
            rows = pl.ds(pl.multiple_of(n * 256, 256), 256)
            dst[:, rows] = src[rows, :].T
            return carry

        lax.fori_loop(0, src.shape[0] // 256, body, 0)

    def turn_weight(i):
        if i == 0:
            need(5)
            turn(down_grad, wd_t)
        elif i == 1:
            need(3)
            turn(gate_grad, wg_t)
        else:
            need(4)
            turn(up_grad, wu_t)

    def scale(r):
        rows = slice(128 * r, 128 * (r + 1))
        cot_rows[rows, :] = (gate_of(r) * cot_rows[rows, :].astype(F32)).astype(BF16)

    def weight_grad(i):
        if i >= 8:
            rows = slice(256 * (i - 8), 256 * (i - 7))
            down_grad[rows, :] = dot(hidden[:, rows], cot_rows[...], 0, 0).astype(BF16)
            return
        out, right = ((gate_grad, d_gate), (up_grad, d_up))[i // 4]

        def body(n, carry):
            rows = pl.ds(pl.multiple_of(512 * (i % 4) + n * 256, 256), 256)
            out[rows, :] = dot(x_t[rows, :], right[...]).astype(BF16)
            return carry

        lax.fori_loop(0, 2, body, 0)

    early = [step for step in PLAN if step[0] == "T"][:3]
    for step in early:
        c = int(step[1])
        pack(index_ref, c // 2, table_ref, c % 2, t_src.at[c])
    lasts = (103, 115)
    for i, step in enumerate(PLAN):
        kind = step[0]
        if step == "bar":
            pl.semaphore_wait(pltpu.get_barrier_semaphore(), 13)
        elif step == "stat":
            norm_statistics()
        elif step == "cot":
            cotangents()
        elif kind == "A":
            hidden_inputs(int(step[1]))
        elif kind == "B":
            slopes(int(step[1]))
        elif kind == "D":
            rest(int(step[1]))
        elif kind == "M":
            turn_weight(int(step[1]))
        elif kind == "S":
            scale(int(step[1]))
        elif kind == "W":
            weight_grad(int(step[1:]))
        else:
            c, d = int(step[1]), step[2]
            part = step[3:]
            done = hops.setdefault((kind, c, part) if part else (kind, c), [])
            k = len(done)
            bufs = families[kind]
            if k:
                done[-1].arrived()
            elif kind == "T" and step not in early:
                pack(index_ref, c // 2, table_ref, c % 2, t_src.at[c])
            elif kind == "C":
                pack_cotangents(c, c_src.at[c])
            if part:
                n = 16 + 2 * c + int(part)
                hop = PartHop(
                    d, int(part), bufs[k].at[c], bufs[k + 1].at[c],
                    (ssem.at[n, k], rsem.at[n, k], lsem.at[n, k]),
                )
            else:
                n = "TC".index(kind) * 8 + c
                hop = Hop(
                    d, AXIS[d], bufs[k].at[c], bufs[k + 1].at[c],
                    (ssem.at[n, k], rsem.at[n, k], lsem.at[n, k]),
                )
            begin(hop)
            done.append(hop)
            if i == 22:
                gate_hops[1].arrived()
                begin(gate_hops[2])
            if i in (lasts[0], lasts[1]):
                slope_hops[lasts.index(i)].arrived()
                begin(slope_hops[lasts.index(i) + 1])
    for c in range(8):
        hops["R", c, "0"][2].arrived()
        hops["R", c, "1"][2].arrived()
    slope_hops[2].arrived()
    for hop in every:
        hop.left()


def finish_kernel(
    spot_any, back_ref, slope_ref, pick_ref, gate_grad, up_grad, down_grad,
    token_out, gates_ref, gate_out, up_out, down_out, spot_ref, token_ref, sums, sem,
):
    copies = []
    for i, (a, b) in enumerate(((gate_grad, gate_out), (up_grad, up_out), (down_grad, down_out))):
        size = a.shape[0] // 4
        for j in range(4):
            part = pl.ds(j * size, size)
            copies.append(pltpu.make_async_copy(a.at[part], b.at[0, part], sem.at[4 * i + j]))
    spots = pltpu.make_async_copy(spot_any, spot_ref, sem.at[12])
    spots.start()
    for copy in copies:
        copy.start()
    spots.wait()

    def body(i, carry):
        for j in range(16):
            t = i * 16 + j
            for h in range(2):
                one = back_ref[spot_ref[0, t] + 128 * h].astype(F32)
                two = back_ref[spot_ref[1, t] + 128 * h].astype(F32)
                sums[h, t] = (one + two).astype(BF16)
        return carry

    lax.fori_loop(0, 8, body, 0)
    perm = to_rows()
    for h in range(2):

        def put(g, b, rows, h=h):
            token_ref[32 * g : 32 * (g + 1), 1024 * h + 128 * b : 1024 * h + 128 * (b + 1)] = rows

        row_pair(perm, lambda g, h=h: sums[h, 32 * g : 32 * (g + 1)].reshape(256, 128), put)
    copies.append(pltpu.make_async_copy(token_ref, token_out, sem.at[13]))
    copies[-1].start()
    slope = slope_ref[:, 0, :].astype(BF16)
    pick = pick_ref[...]
    lane = iota((128, 128), 1)
    lane_f = lane.astype(F32)
    both = jnp.zeros((128, 128), F32)
    for k in range(2):
        one = (pick[:, 2 + k : 3 + k] == lane_f).astype(F32).astype(BF16)
        mine = jnp.where(lane_f == pick[:, 4 + k : 5 + k], dot(one, slope), 0.0)
        both = jnp.where(lane == k, jnp.sum(mine, axis=1, keepdims=True), both)
    gates_ref[...] = both.T[:2].astype(BF16)
    for copy in copies:
        copy.wait()


def struct(shape, dtype=BF16):
    return jax.ShapeDtypeStruct(shape, dtype)


def local(tokens, routes, gates, w_gate, w_up, w_down, moe_out, norm_gain, out_grad):
    pieces = (8, 4, 4, 8, 8, 128)
    halves = (8, 4, 4, 4, 2, 8, 128)
    lanes = (4, 4, 8, 1, 128)
    deep, flat = (2048, 768), (768, 2048)
    rows, inner = (512, 2048), (512, 768)
    back, slope, spot, pick, gate_grad, up_grad, down_grad = pl.pallas_call(
        mega_kernel,
        out_shape=(
            pltpu.VMEM(halves, BF16),
            pltpu.VMEM(lanes, F32),
            pltpu.VMEM((8, 128), jnp.int32),
            pltpu.VMEM((128, 128), F32),
            pltpu.VMEM(deep, BF16),
            pltpu.VMEM(deep, BF16),
            pltpu.VMEM(flat, BF16),
        ),
        in_specs=[VMEM] * 3 + [ANY] * 6,
        out_specs=(VMEM,) * 7,
        scratch_shapes=[
            pltpu.VMEM((128, 2048), BF16),
            pltpu.VMEM((1024, 256), BF16),
            pltpu.VMEM((1024, 256), BF16),
            pltpu.VMEM((8, 128), jnp.int32),
            pltpu.SMEM((8, 128), jnp.int32),
            pltpu.VMEM(lanes, F32),
            pltpu.VMEM((2, 129, 8, 128), BF16),
            pltpu.VMEM((3, 8, 128), F32),
            pltpu.VMEM(flat, BF16),
            pltpu.VMEM(flat, BF16),
            pltpu.VMEM(deep, BF16),
            *[pltpu.VMEM(pieces, BF16)] * 8,
            *[pltpu.VMEM(halves, BF16)] * 3,
            *[pltpu.VMEM(lanes, F32)] * 6,
            pltpu.VMEM((8, 3, 8, 128), F32),
            pltpu.VMEM((8, 128, 256), BF16),
            pltpu.VMEM((128, 128), F32),
            pltpu.VMEM((128, 128), F32),
            pltpu.VMEM((128, 2048), BF16),
            pltpu.VMEM((2048, 512), BF16),
            pltpu.VMEM(inner, BF16),
            pltpu.VMEM(inner, BF16),
            pltpu.VMEM(inner, BF16),
            pltpu.VMEM((4, 128, 768), F32),
            pltpu.VMEM((4, 128, 768), F32),
            pltpu.VMEM(rows, BF16),
            pltpu.VMEM((128, 1024), BF16),
            pltpu.VMEM((128, 128), F32),
            pltpu.SemaphoreType.DMA((32, 3)),
            pltpu.SemaphoreType.DMA((32, 3)),
            pltpu.SemaphoreType.DMA((32, 3)),
            pltpu.SemaphoreType.DMA((8, 3)),
            pltpu.SemaphoreType.DMA((7,)),
        ],
        compiler_params=pltpu.CompilerParams(
            collective_id=0, has_side_effects=True, vmem_limit_bytes=48 << 20
        ),
        name="exchange",
    )(
        routes.T, gates.T, norm_gain.reshape(1, 256), tokens, moe_out, out_grad,
        w_gate[0], w_up[0], w_down[0],
    )
    token_grad, gates_grad, *grads = pl.pallas_call(
        finish_kernel,
        out_shape=(
            struct((128, 2048)),
            struct((2, 128)),
            struct((1, *deep)),
            struct((1, *deep)),
            struct((1, *flat)),
        ),
        in_specs=[VMEM] * 7,
        out_specs=(ANY, VMEM, ANY, ANY, ANY),
        scratch_shapes=[
            pltpu.SMEM((8, 128), jnp.int32),
            pltpu.VMEM((128, 2048), BF16),
            pltpu.VMEM((2, 128, 8, 128), BF16),
            pltpu.SemaphoreType.DMA((14,)),
        ],
        compiler_params=pltpu.CompilerParams(vmem_limit_bytes=8 << 20),
        name="finish",
    )(spot, back.reshape(1024, 8, 128), slope.reshape(128, 1, 128), pick, gate_grad, up_grad, down_grad)
    return (token_grad, gates_grad.T, *grads)


def solution(mesh):
    split = P(("ep", "tp"), None)
    expert = P(("ep", "tp"), None, None)
    in_specs = (split, split, split, expert, expert, expert, P("ep", "tp"), P("tp"), P("ep", "tp"))
    out_specs = (split, split, expert, expert, expert)
    return jax.shard_map(local, mesh=mesh, in_specs=in_specs, out_specs=out_specs, check_vma=False)
```

```python
import jax
import jax.numpy as jnp
from jax import lax
from jax.experimental import pallas as pl
from jax.experimental.pallas import tpu as pltpu
from jax.sharding import PartitionSpec as P

F32 = jnp.float32
BF16 = jnp.bfloat16
MESH = pl.DeviceIdType.MESH
VMEM = pl.BlockSpec(memory_space=pltpu.VMEM)
SMEM = pl.BlockSpec(memory_space=pltpu.SMEM)
ANY = pl.BlockSpec(memory_space=pl.ANY)
SIZE = {"z": 4, "x": 4, "t": 8}
AXIS = {"z": 0, "x": 1, "t": 2}
epsilon = 1e-06

PLAN = (
    "bar", "stat", "T1x", "T0z", "T3t", "T7z", "T6x", "T2z", "T4t", "T5x", "T1t", "cot",
    "C6z", "C5t", "C4x", "C7z", "C2t", "T4x", "C1t", "T5z", "T7x", "M1", "C4t", "C0x",
    "C6t", "C5z", "T6z", "C7x", "T4z", "T5t", "M0", "C1x", "C4z", "C0z", "M2", "C5x",
    "T0x", "T7t", "C6x", "C3z", "T1z", "C2x", "T6t", "C7t", "T2t", "A2", "B2", "D2",
    "R5z1", "T0t", "T3x", "C1z", "A3", "S2", "C3x", "C0t", "B3", "R6z0", "D3", "R7t0",
    "R7x1", "R6t1", "T3z", "T2x", "R4z1", "C2z", "R4x0", "A0", "R6t0", "R5x0", "C3t", "B0",
    "R0z0", "R0t1", "R7t1", "R6x1", "D0", "R1z1", "R1z0", "R4t1", "R6x0", "A1", "R5z0", "R7x0",
    "R4t0", "R5x1", "B1", "R2x0", "R2t1", "R6z1", "D1", "S1", "R3x0", "R3z1", "R0t0", "W6",
    "R0x1", "R7z1", "W5", "R7z0", "R1t1", "R4x1", "W1", "R2t0", "S0", "R2z1", "R1x0", "R3t0",
    "W2", "R3x1", "R4z0", "R5t0", "R0x0", "W3", "R5t1", "R0z1", "R2z0", "R1x1", "R1t0", "R2x1",
    "S3", "R3z0", "R3t1", "W9", "W7", "W4", "W10", "W0", "W8",
)


def iota(shape, dim):
    return lax.broadcasted_iota(jnp.int32, shape, dim)


def dot(a, b, a_dim=1, b_dim=0):
    return lax.dot_general(
        a, b, (((a_dim,), (b_dim,)), ((), ())), preferred_element_type=F32
    )


def to_rows():
    i, j = iota((256, 256), 0), iota((256, 256), 1)
    return (((i >> 5) == (j & 7)) & ((i & 31) == (j >> 3))).astype(F32).astype(BF16)


def to_tiles():
    i, j = iota((256, 256), 0), iota((256, 256), 1)
    return (((i >> 3) == (j & 31)) & ((i & 7) == (j >> 5))).astype(F32).astype(BF16)


def to_expert_rows():
    i, j = iota((256, 256), 0), iota((256, 256), 1)
    place = (((i >> 2) & 3) << 3) | (((i >> 4) & 1) << 2) | (i & 3)
    return (j == ((place << 3) | (i >> 5))).astype(F32).astype(BF16)


def from_expert_rows():
    j, i = iota((256, 256), 0), iota((256, 256), 1)
    place = (((i >> 2) & 3) << 3) | (((i >> 4) & 1) << 2) | (i & 3)
    return (j == ((place << 3) | (i >> 5))).astype(F32).astype(BF16)


def to_expert_cols():
    i, j = iota((256, 256), 0), iota((256, 256), 1)
    spot = (((i >> 2) & 3) << 6) | ((i >> 5) << 3) | ((i & 3) << 1) | ((i >> 4) & 1)
    return (j == spot).astype(F32).astype(BF16)


def expert_order():
    i, j = iota((128, 128), 0), iota((128, 128), 1)
    place = ((i >> 5) << 5) | (((i >> 2) & 3) << 3) | (((i >> 4) & 1) << 2) | (i & 3)
    return (j == place).astype(F32).astype(BF16)


def tile_pair(perm, pieces, put):
    for pair in range(2):
        both = jnp.concatenate(
            [jnp.concatenate(pieces(2 * pair + j), axis=0) for j in range(2)], axis=1
        )
        out = dot(perm, both).astype(BF16)
        for j in range(2):
            put(2 * pair + j, out[:, 128 * j : 128 * (j + 1)])


def row_pair(perm, tiles, put):
    for pair in range(2):
        both = jnp.concatenate([tiles(2 * pair + j) for j in range(2)], axis=1)
        out = dot(perm, both).astype(BF16)
        for j in range(2):
            for b in range(8):
                put(2 * pair + j, b, out[32 * b : 32 * (b + 1), 128 * j : 128 * (j + 1)])


def statistics(moe, grad, gain_ref, stat_ref):
    for b in range(8):
        rows = slice(128 * b, 128 * (b + 1))
        saved = moe[rows, :].astype(F32)
        scaled = gain_ref[...] * grad[rows, :].astype(F32)
        for s, prod in enumerate((saved * saved, saved * scaled)):
            part = (prod[:, :128] + prod[:, 128:]).T
            stat_ref[s, b : b + 1, :] = jnp.sum(part, axis=0, keepdims=True)


def routing(routes_ref, gates_ref, index_ref, stat_ref, spot_ref, gate_ref, pick_ref):
    head = jnp.concatenate(
        [routes_ref[...].astype(F32), gates_ref[...], jnp.zeros((4, 128), F32)], axis=0
    )
    cols = head.T
    lane, row = iota((128, 128), 1), iota((128, 128), 0)
    lane_f = lane.astype(F32)
    below = (lane < row).astype(F32).astype(BF16)
    hot = [(cols[:, k : k + 1] == lane_f).astype(F32) for k in range(2)]
    seen = dot(below, (hot[0] + hot[1]).astype(BF16))
    rank = [jnp.sum(hot[k] * seen, axis=1, keepdims=True) for k in range(2)]
    number = (row + 1).astype(F32)
    index = jnp.zeros((128, 128), F32)
    gate = jnp.zeros((128, 128), F32)
    for k in range(2):
        at = lane_f == rank[k]
        one = hot[k].astype(BF16)
        index += dot(jnp.where(at, number, 0.0).astype(BF16), one, 0, 0)
        gate += dot(one, jnp.where(at, cols[:, 2 + k : 3 + k], 0.0).astype(BF16), 0, 0)
    index_ref[...] = jnp.clip(index[:8].astype(jnp.int32), 0, 128)
    stat_ref[2] = index[:8]
    for z in range(4):
        for x in range(4):
            gate_ref[z, x, :, 0, :] = gate[32 * z + 8 * x : 32 * z + 8 * x + 8, :]
    pick = jnp.zeros((128, 128), F32)
    for k in range(2):
        pick = jnp.where(lane == k, rank[k] * 256.0 + cols[:, k : k + 1], pick)
        pick = jnp.where(lane == 2 + k, cols[:, k : k + 1], pick)
        pick = jnp.where(lane == 4 + k, rank[k], pick)
    pick_ref[...] = pick
    spot_ref[...] = pick.T[:8].astype(jnp.int32)


def token_table(perm, tokens, table_ref):
    for h in range(2):
        table_ref[h, 0] = jnp.zeros((8, 128), BF16)

        def pieces(g, h=h):
            return [
                tokens[32 * g : 32 * (g + 1), 1024 * h + 128 * b : 1024 * h + 128 * (b + 1)]
                for b in range(8)
            ]

        def put(g, tiles, h=h):
            table_ref[h, 1 + 32 * g : 33 + 32 * g] = tiles.reshape(32, 8, 128)

        tile_pair(perm, pieces, put)


def coords():
    ep = lax.axis_index("ep")
    return {"z": ep // 4, "x": ep % 4, "t": lax.axis_index("tp")}


def peers(dim, here):
    if dim != "t":
        return [(here + k) % 4 for k in (2, 1, 3)]
    return [
        (here // 2 + dy) % 4 * 2 + (here % 2 + dc) % 2
        for dy, dc in ((2, 0), (2, 1), (1, 0), (3, 0), (1, 1), (3, 1), (0, 1))
    ]


def others():
    me = coords()
    for dim in "zxt":
        for p in peers(dim, me[dim]):
            place = {**me, dim: p}
            yield dim, p, (place["z"] * 4 + place["x"], place["t"])


def greet():
    for _, _, device in others():
        pl.semaphore_signal(
            pltpu.get_barrier_semaphore(), inc=1, device_id=device, device_id_type=MESH
        )


def cut(ref, axis, index):
    return ref.at[(slice(None),) * axis + (index,)]


class Hop:
    def __init__(self, dim, axis, src, dst, sems, whole=False):
        self.dim, self.axis, self.whole, self.gone = dim, axis, whole, False
        self.src, self.dst, (self.ssem, self.rsem, self.lsem) = src, dst, sems

    def piece(self, index):
        return self.src if self.whole else cut(self.src, self.axis, index)

    def start(self):
        mine = coords()[self.dim]
        for dim, p, device in others():
            if dim == self.dim:
                pltpu.make_async_remote_copy(
                    self.piece(p),
                    cut(self.dst, self.axis, mine),
                    self.ssem,
                    self.rsem,
                    device_id=device,
                    device_id_type=MESH,
                ).start()
        pltpu.make_async_copy(self.piece(mine), cut(self.dst, self.axis, mine), self.lsem).start()

    def remote_part(self):
        return cut(self.dst, self.axis, slice(0, SIZE[self.dim] - 1))

    def arrived(self):
        part = self.remote_part()
        pltpu.make_async_copy(part, part, self.rsem).wait()
        one = cut(self.dst, self.axis, 0)
        pltpu.make_async_copy(one, one, self.lsem).wait()

    def left(self):
        if self.gone:
            return
        self.gone = True
        part = self.remote_part()
        pltpu.make_async_copy(part, part, self.ssem).wait()


class PartHop(Hop):
    def __init__(self, dim, part, src, dst, sems):
        core = lax.axis_index("tp") % 2
        kind = core if part == 0 else 1 - core
        self.cross = dim == "t" and part == 1
        self.far = dst.at[:, :, :, 1 - kind]
        src, dst = src.at[:, :, :, kind], dst.at[:, :, :, kind]
        super().__init__(dim, AXIS[dim], src, dst, sems)

    def start(self):
        if self.dim != "t":
            super().start()
            return
        me = coords()
        mine, core = me["t"] // 2, me["t"] % 2
        for k in (2, 1, 3, 0) if self.cross else (2, 1, 3):
            p = (mine + k) % 4
            place = 2 * p + (1 - core if self.cross else core)
            pltpu.make_async_remote_copy(
                cut(self.src, 2, p),
                cut(self.far if self.cross else self.dst, 2, mine),
                self.ssem,
                self.rsem,
                device_id=(me["z"] * 4 + me["x"], place),
                device_id_type=MESH,
            ).start()
        if not self.cross:
            pltpu.make_async_copy(cut(self.src, 2, mine), cut(self.dst, 2, mine), self.lsem).start()

    def remote_part(self):
        return self.dst if self.cross else cut(self.dst, self.axis, slice(0, 3))

    def arrived(self):
        if self.cross:
            pltpu.make_async_copy(self.dst, self.dst, self.rsem).wait()
        else:
            super().arrived()


def pack(index_ref, rank, table_ref, half, dst):
    def body(i, carry):
        for t in range(8):
            dst[i // 4, i % 4, t] = table_ref[half, index_ref[rank, i * 8 + t]]
        return carry

    lax.fori_loop(0, 16, body, 0)


def mega_kernel(
    routes_any, gates_any, gain_any, tokens_any, moe_any, grad_any, wg_any, wu_any, wd_any,
    back_ref, slope_ref, spot_ref, pick_ref, gate_grad, up_grad, down_grad,
    routes_ref, gates_ref, gain_ref, tokens, moe, grad, index_v, index_ref, gate_src, table_ref, stat_ref,
    wg_t, wu_t, wd_t, t_src, t_one, t_two, t_out, c_src, c_one, c_two, c_out, r_src, r_one, r_two,
    g_one, g_two, g_out, q_src, q_one, q_two, s_in, cot_parts, index_cols, gate_cols,
    x_rows, x_t, d_gate, d_up, hidden, pre_gate, pre_up, cot_rows, back_rows, slope,
    ssem, rsem, lsem, misc, wsem,
):
    wg, wu = gate_grad, up_grad
    loads = [
        pltpu.make_async_copy(a, b, wsem.at[i])
        for i, (a, b) in enumerate(
            (
                (moe_any, moe), (grad_any, grad), (tokens_any, tokens),
                (wg_any, gate_grad), (wu_any, up_grad), (wd_any, down_grad),
                (routes_any, routes_ref), (gates_any, gates_ref), (gain_any, gain_ref),
            )
        )
    ]
    loaded = set()

    def need(*which):
        for i in which:
            if i not in loaded:
                loads[i].wait()
                loaded.add(i)

    greet()
    for i in (6, 7, 8, 0, 1, 2, 3, 4, 5):
        loads[i].start()
    slope[...] = jnp.zeros((128, 128), F32)
    need(6, 7, 8)
    routing(routes_ref, gates_ref, index_v, stat_ref, spot_ref, gate_src, pick_ref)
    index_copy = pltpu.make_async_copy(index_v, index_ref, wsem.at[9])
    index_copy.start()
    need(0, 1)
    statistics(moe, grad, gain_ref, stat_ref)
    need(2)
    token_table(to_tiles(), tokens, table_ref)
    index_copy.wait()
    families = {
        "T": (t_src, t_one, t_two, t_out),
        "C": (c_src, c_one, c_two, c_out),
        "R": (r_src, r_one, r_two, back_ref),
    }
    hops = {}
    every = []

    def small(i):
        return tuple(misc.at[i, j] for j in range(3))

    stat_hop = Hop("t", 0, stat_ref, s_in, small(0), whole=True)
    gate_hops = [
        Hop(d, AXIS[d], a, b, small(2 + i))
        for i, (d, a, b) in enumerate(
            (("x", gate_src, g_one), ("t", g_one, g_two), ("z", g_two, g_out))
        )
    ]
    slope_hops = [
        Hop(d, AXIS[d], a, b, small(5 + i))
        for i, (d, a, b) in enumerate(
            (("x", q_src, q_one), ("t", q_one, q_two), ("z", q_two, slope_ref))
        )
    ]

    def begin(hop):
        hop.start()
        every.append(hop)

    def norm_statistics():
        begin(stat_hop)
        begin(gate_hops[0])

    def cotangents():
        stat_hop.arrived()
        total = s_in[0]
        for p in range(1, 8):
            total += s_in[p]
        inv = lax.rsqrt(total[0] / 2048.0 + epsilon)
        cols = jnp.concatenate([inv, inv**3 * total[1] / 2048.0], axis=0).T

        for b in range(8):
            rows = slice(128 * b, 128 * (b + 1))
            scaled = gain_ref[...] * grad[rows, :].astype(F32)
            saved = moe[rows, :].astype(F32)
            cot_parts[b] = (
                cols[:, b : b + 1] * scaled - saved * cols[:, 8 + b : 9 + b]
            ).astype(BF16)
        index_cols[...] = jnp.concatenate(
            [s_in[b, 2] for b in range(8)] + [jnp.zeros((64, 128), F32)], axis=0
        ).T
        gate_hops[0].arrived()
        begin(gate_hops[1])

    def pack_cotangents(c, dst):
        rank, half = c // 2, c % 2
        number = (iota((128, 128), 1) + 1).astype(F32)
        parts = []
        for b in range(4 * half, 4 * half + 4):
            index = index_cols[:, 8 * b + rank : 8 * b + rank + 1]
            chosen = (index == number).astype(F32).astype(BF16)
            parts.append(dot(chosen, cot_parts[b]).astype(BF16))

        def pieces(g):
            return [
                part[32 * g : 32 * (g + 1), 128 * b : 128 * (b + 1)]
                for part in parts
                for b in range(2)
            ]

        def put(g, tiles):
            dst[g] = tiles.reshape(4, 8, 8, 128)

        tile_pair(to_tiles(), pieces, put)

    def unpack(src, dst, row, half):
        def put(g, b, rows):
            dst[
                row + 32 * g : row + 32 * (g + 1), 1024 * half + 128 * b : 1024 * half + 128 * b + 128
            ] = rows

        row_pair(to_expert_rows(), lambda g: src[g].reshape(256, 128), put)

    def unpack_cotangents(src, row, half):
        perm = to_expert_cols()
        for pair in range(2):
            both = jnp.concatenate([src[2 * pair + j].reshape(256, 128) for j in range(2)], axis=1)
            out = dot(perm, both).astype(BF16)
            for j in range(2):
                at = row + 32 * (2 * pair + j) + 16 * half
                for b in range(16):
                    cot_rows[at : at + 16, 128 * b : 128 * (b + 1)] = out[
                        16 * b : 16 * (b + 1), 128 * j : 128 * (j + 1)
                    ]

    def hidden_inputs(r):
        need(3, 4)
        for h in range(2):
            hops["T", 2 * r + h][2].arrived()
            unpack(t_out.at[2 * r + h], x_rows, 0, h)

        def body(n, carry):
            cols = pl.ds(pl.multiple_of(n * 256, 256), 256)
            x = x_rows[...]
            pre_gate[r, :, cols] = dot(x, wg[:, cols])
            pre_up[r, :, cols] = dot(x, wu[:, cols])
            return carry

        lax.fori_loop(0, 3, body, 0)

        def turned(n, carry):
            cols = pl.ds(pl.multiple_of(n * 256, 256), 256)
            x_t[cols, 128 * r : 128 * (r + 1)] = x_rows[:, cols].T
            return carry

        lax.fori_loop(0, 8, turned, 0)

    def half_back(r, h):
        rows = slice(128 * r, 128 * (r + 1))

        def body(n, carry):
            wide = pl.ds(pl.multiple_of(1024 * h + n * 512, 512), 512)
            total = dot(d_gate[rows, :], wg_t[:, wide]) + dot(d_up[rows, :], wu_t[:, wide])
            back_rows[:, pl.ds(pl.multiple_of(n * 512, 512), 512)] = total.astype(BF16)
            return carry

        lax.fori_loop(0, 2, body, 0)

        def pieces(g):
            return [
                back_rows[32 * g : 32 * (g + 1), 128 * b : 128 * (b + 1)] for b in range(8)
            ]

        def put(g, tiles):
            r_src[2 * r + h, g] = tiles.reshape(4, 4, 2, 8, 128)

        tile_pair(from_expert_rows(), pieces, put)

    def gate_of(r):
        return gate_cols[:, r : r + 1]

    def slopes(r):
        if r == 2:
            gate_hops[2].arrived()
            gates = jnp.concatenate(
                [g_out[z, x][:, 0, :] for z in range(4) for x in range(4)], axis=0
            )
            gate_cols[...] = dot(expert_order(), gates.astype(BF16))
        for h in range(2):
            hops["C", 2 * r + h][2].arrived()
            unpack_cotangents(c_out.at[2 * r + h], 128 * r, h)
        gate = gate_of(r)
        rows = slice(128 * r, 128 * (r + 1))

        def body(n, carry):
            cols = pl.ds(pl.multiple_of(n * 256, 256), 256)
            hid_grad = dot(cot_rows[rows, :], wd_t[:, cols])
            p_gate, p_up = pre_gate[r, :, cols], pre_up[r, :, cols]
            sig = jax.nn.sigmoid(p_gate)
            act = p_gate * sig
            hid = act * p_up
            d_hid = gate * hid_grad
            d_gate[rows, cols] = (d_hid * p_up * sig * (1.0 + p_gate * (1.0 - sig))).astype(BF16)
            d_up[rows, cols] = (d_hid * act).astype(BF16)
            hidden[rows, cols] = hid.astype(BF16)
            return carry + jnp.sum(hid * hid_grad, axis=1, keepdims=True)

        total = lax.fori_loop(0, 3, body, jnp.zeros((128, 1), F32))
        slope[...] = jnp.where(iota((128, 128), 1) == r, total, slope[...])
        half_back(r, 0)

    def rest(r):
        half_back(r, 1)
        if r == 1:
            slope[...] = dot(expert_order(), slope[...].astype(BF16), 0, 0)
            for z in range(4):
                for x in range(4):
                    q_src[z, x, :, 0, :] = slope[32 * z + 8 * x : 32 * z + 8 * x + 8, :]
            begin(slope_hops[0])

    def turn(src, dst):
        def body(n, carry):
            rows = pl.ds(pl.multiple_of(n * 256, 256), 256)
            dst[:, rows] = src[rows, :].T
            return carry

        lax.fori_loop(0, src.shape[0] // 256, body, 0)

    def turn_weight(i):
        if i == 0:
            need(5)
            turn(down_grad, wd_t)
        elif i == 1:
            need(3)
            turn(gate_grad, wg_t)
        else:
            need(4)
            turn(up_grad, wu_t)

    def scale(r):
        rows = slice(128 * r, 128 * (r + 1))
        cot_rows[rows, :] = (gate_of(r) * cot_rows[rows, :].astype(F32)).astype(BF16)

    def weight_grad(i):
        if i >= 8:
            rows = slice(256 * (i - 8), 256 * (i - 7))
            down_grad[rows, :] = dot(hidden[:, rows], cot_rows[...], 0, 0).astype(BF16)
            return
        out, right = ((gate_grad, d_gate), (up_grad, d_up))[i // 4]

        def body(n, carry):
            rows = pl.ds(pl.multiple_of(512 * (i % 4) + n * 256, 256), 256)
            out[rows, :] = dot(x_t[rows, :], right[...]).astype(BF16)
            return carry

        lax.fori_loop(0, 2, body, 0)

    early = [step for step in PLAN if step[0] == "T"][:3]
    for step in early:
        c = int(step[1])
        pack(index_ref, c // 2, table_ref, c % 2, t_src.at[c])
    lasts = (103, 115)
    for i, step in enumerate(PLAN):
        kind = step[0]
        if step == "bar":
            pl.semaphore_wait(pltpu.get_barrier_semaphore(), 13)
        elif step == "stat":
            norm_statistics()
        elif step == "cot":
            cotangents()
        elif kind == "A":
            hidden_inputs(int(step[1]))
        elif kind == "B":
            slopes(int(step[1]))
        elif kind == "D":
            rest(int(step[1]))
        elif kind == "M":
            turn_weight(int(step[1]))
        elif kind == "S":
            scale(int(step[1]))
        elif kind == "W":
            weight_grad(int(step[1:]))
        else:
            c, d = int(step[1]), step[2]
            part = step[3:]
            done = hops.setdefault((kind, c, part) if part else (kind, c), [])
            k = len(done)
            bufs = families[kind]
            if k:
                done[-1].arrived()
            elif kind == "T" and step not in early:
                pack(index_ref, c // 2, table_ref, c % 2, t_src.at[c])
            elif kind == "C":
                pack_cotangents(c, c_src.at[c])
            if part:
                n = 16 + 2 * c + int(part)
                hop = PartHop(
                    d, int(part), bufs[k].at[c], bufs[k + 1].at[c],
                    (ssem.at[n, k], rsem.at[n, k], lsem.at[n, k]),
                )
            else:
                n = "TC".index(kind) * 8 + c
                hop = Hop(
                    d, AXIS[d], bufs[k].at[c], bufs[k + 1].at[c],
                    (ssem.at[n, k], rsem.at[n, k], lsem.at[n, k]),
                )
            begin(hop)
            done.append(hop)
            if i == 22:
                gate_hops[1].arrived()
                begin(gate_hops[2])
            if i in (lasts[0], lasts[1]):
                slope_hops[lasts.index(i)].arrived()
                begin(slope_hops[lasts.index(i) + 1])
    for c in range(8):
        hops["R", c, "0"][2].arrived()
        hops["R", c, "1"][2].arrived()
    slope_hops[2].arrived()
    for hop in every:
        hop.left()


def finish_kernel(
    spot_any, back_ref, slope_ref, pick_ref, gate_grad, up_grad, down_grad,
    token_out, gates_ref, gate_out, up_out, down_out, spot_ref, token_ref, sums, sem,
):
    copies = []
    for i, (a, b) in enumerate(((gate_grad, gate_out), (up_grad, up_out), (down_grad, down_out))):
        size = a.shape[0] // 4
        for j in range(4):
            part = pl.ds(j * size, size)
            copies.append(pltpu.make_async_copy(a.at[part], b.at[0, part], sem.at[4 * i + j]))
    spots = pltpu.make_async_copy(spot_any, spot_ref, sem.at[12])
    spots.start()
    for copy in copies:
        copy.start()
    spots.wait()

    def body(i, carry):
        for j in range(16):
            t = i * 16 + j
            for h in range(2):
                one = back_ref[spot_ref[0, t] + 128 * h].astype(F32)
                two = back_ref[spot_ref[1, t] + 128 * h].astype(F32)
                sums[h, t] = (one + two).astype(BF16)
        return carry

    lax.fori_loop(0, 8, body, 0)
    perm = to_rows()
    for h in range(2):

        def put(g, b, rows, h=h):
            token_ref[32 * g : 32 * (g + 1), 1024 * h + 128 * b : 1024 * h + 128 * (b + 1)] = rows

        row_pair(perm, lambda g, h=h: sums[h, 32 * g : 32 * (g + 1)].reshape(256, 128), put)
    copies.append(pltpu.make_async_copy(token_ref, token_out, sem.at[13]))
    copies[-1].start()
    slope = slope_ref[:, 0, :].astype(BF16)
    pick = pick_ref[...]
    lane = iota((128, 128), 1)
    lane_f = lane.astype(F32)
    both = jnp.zeros((128, 128), F32)
    for k in range(2):
        one = (pick[:, 2 + k : 3 + k] == lane_f).astype(F32).astype(BF16)
        mine = jnp.where(lane_f == pick[:, 4 + k : 5 + k], dot(one, slope), 0.0)
        both = jnp.where(lane == k, jnp.sum(mine, axis=1, keepdims=True), both)
    gates_ref[...] = both.T[:2].astype(BF16)
    for copy in copies:
        copy.wait()


def struct(shape, dtype=BF16):
    return jax.ShapeDtypeStruct(shape, dtype)


def local(tokens, routes, gates, w_gate, w_up, w_down, moe_out, norm_gain, out_grad):
    pieces = (8, 4, 4, 8, 8, 128)
    halves = (8, 4, 4, 4, 2, 8, 128)
    lanes = (4, 4, 8, 1, 128)
    deep, flat = (2048, 768), (768, 2048)
    rows, inner = (512, 2048), (512, 768)
    back, slope, spot, pick, gate_grad, up_grad, down_grad = pl.pallas_call(
        mega_kernel,
        out_shape=(
            pltpu.VMEM(halves, BF16),
            pltpu.VMEM(lanes, F32),
            pltpu.VMEM((8, 128), jnp.int32),
            pltpu.VMEM((128, 128), F32),
            pltpu.VMEM(deep, BF16),
            pltpu.VMEM(deep, BF16),
            pltpu.VMEM(flat, BF16),
        ),
        in_specs=[ANY] * 9,
        out_specs=(VMEM,) * 7,
        scratch_shapes=[
            pltpu.VMEM((2, 128), jnp.int32),
            pltpu.VMEM((2, 128), F32),
            pltpu.VMEM((1, 256), F32),
            pltpu.VMEM((128, 2048), BF16),
            pltpu.VMEM((1024, 256), BF16),
            pltpu.VMEM((1024, 256), BF16),
            pltpu.VMEM((8, 128), jnp.int32),
            pltpu.SMEM((8, 128), jnp.int32),
            pltpu.VMEM(lanes, F32),
            pltpu.VMEM((2, 129, 8, 128), BF16),
            pltpu.VMEM((3, 8, 128), F32),
            pltpu.VMEM(flat, BF16),
            pltpu.VMEM(flat, BF16),
            pltpu.VMEM(deep, BF16),
            *[pltpu.VMEM(pieces, BF16)] * 8,
            *[pltpu.VMEM(halves, BF16)] * 3,
            *[pltpu.VMEM(lanes, F32)] * 6,
            pltpu.VMEM((8, 3, 8, 128), F32),
            pltpu.VMEM((8, 128, 256), BF16),
            pltpu.VMEM((128, 128), F32),
            pltpu.VMEM((128, 128), F32),
            pltpu.VMEM((128, 2048), BF16),
            pltpu.VMEM((2048, 512), BF16),
            pltpu.VMEM(inner, BF16),
            pltpu.VMEM(inner, BF16),
            pltpu.VMEM(inner, BF16),
            pltpu.VMEM((4, 128, 768), F32),
            pltpu.VMEM((4, 128, 768), F32),
            pltpu.VMEM(rows, BF16),
            pltpu.VMEM((128, 1024), BF16),
            pltpu.VMEM((128, 128), F32),
            pltpu.SemaphoreType.DMA((32, 3)),
            pltpu.SemaphoreType.DMA((32, 3)),
            pltpu.SemaphoreType.DMA((32, 3)),
            pltpu.SemaphoreType.DMA((8, 3)),
            pltpu.SemaphoreType.DMA((10,)),
        ],
        compiler_params=pltpu.CompilerParams(
            collective_id=0, has_side_effects=True, vmem_limit_bytes=48 << 20
        ),
        name="exchange",
    )(
        routes.T, gates.T, norm_gain.reshape(1, 256), tokens, moe_out, out_grad,
        w_gate[0], w_up[0], w_down[0],
    )
    token_grad, gates_grad, *grads = pl.pallas_call(
        finish_kernel,
        out_shape=(
            struct((128, 2048)),
            struct((2, 128)),
            struct((1, *deep)),
            struct((1, *deep)),
            struct((1, *flat)),
        ),
        in_specs=[VMEM] * 7,
        out_specs=(ANY, VMEM, ANY, ANY, ANY),
        scratch_shapes=[
            pltpu.SMEM((8, 128), jnp.int32),
            pltpu.VMEM((128, 2048), BF16),
            pltpu.VMEM((2, 128, 8, 128), BF16),
            pltpu.SemaphoreType.DMA((14,)),
        ],
        compiler_params=pltpu.CompilerParams(vmem_limit_bytes=8 << 20),
        name="finish",
    )(spot, back.reshape(1024, 8, 128), slope.reshape(128, 1, 128), pick, gate_grad, up_grad, down_grad)
    return (token_grad, gates_grad.T, *grads)


def solution(mesh):
    split = P(("ep", "tp"), None)
    expert = P(("ep", "tp"), None, None)
    in_specs = (split, split, split, expert, expert, expert, P("ep", "tp"), P("tp"), P("ep", "tp"))
    out_specs = (split, split, expert, expert, expert)
    return jax.shard_map(local, mesh=mesh, in_specs=in_specs, out_specs=out_specs, check_vma=False)
```

```python
import jax
import jax.numpy as jnp
from jax import lax
from jax.experimental import pallas as pl
from jax.experimental.pallas import tpu as pltpu
from jax.sharding import PartitionSpec as P

F32 = jnp.float32
BF16 = jnp.bfloat16
MESH = pl.DeviceIdType.MESH
VMEM = pl.BlockSpec(memory_space=pltpu.VMEM)
SMEM = pl.BlockSpec(memory_space=pltpu.SMEM)
ANY = pl.BlockSpec(memory_space=pl.ANY)
SIZE = {"z": 4, "x": 4, "t": 8}
AXIS = {"z": 0, "x": 1, "t": 2}
epsilon = 1e-06

PLAN = (
    "bar", "stat", "T1x", "T0z", "T3t", "T7z", "T6x", "T2z", "T4t", "T5x", "T1t", "cot",
    "C6z", "C5t", "C4x", "C7z", "C2t", "T4x", "C1t", "T5z", "T7x", "M1", "C4t", "C0x",
    "C6t", "C5z", "T6z", "C7x", "T4z", "T5t", "M0", "C1x", "C4z", "C0z", "M2", "C5x",
    "T0x", "T7t", "C6x", "C3z", "T1z", "C2x", "T6t", "C7t", "T2t", "A2", "B2", "D2",
    "R5z1", "T0t", "T3x", "C1z", "A3", "S2", "C3x", "C0t", "B3", "R6z0", "D3", "R7t0",
    "R7x1", "R6t1", "T3z", "T2x", "R4z1", "C2z", "R4x0", "A0", "R6t0", "R5x0", "C3t", "B0",
    "R0z0", "R0t1", "R7t1", "R6x1", "D0", "R1z1", "R1z0", "R4t1", "R6x0", "A1", "R5z0", "R7x0",
    "R4t0", "R5x1", "B1", "R2x0", "R2t1", "R6z1", "D1", "S1", "R3x0", "R3z1", "R0t0", "W6",
    "R0x1", "R7z1", "W5", "R7z0", "R1t1", "R4x1", "W1", "R2t0", "S0", "R2z1", "R1x0", "R3t0",
    "W2", "R3x1", "R4z0", "R5t0", "R0x0", "W3", "R5t1", "R0z1", "R2z0", "R1x1", "R1t0", "R2x1",
    "S3", "R3z0", "R3t1", "W9", "W7", "W4", "W10", "W0", "W8",
)


def iota(shape, dim):
    return lax.broadcasted_iota(jnp.int32, shape, dim)


def dot(a, b, a_dim=1, b_dim=0):
    return lax.dot_general(
        a, b, (((a_dim,), (b_dim,)), ((), ())), preferred_element_type=F32
    )


def to_rows():
    i, j = iota((256, 256), 0), iota((256, 256), 1)
    return (((i >> 5) == (j & 7)) & ((i & 31) == (j >> 3))).astype(F32).astype(BF16)


def to_tiles():
    i, j = iota((256, 256), 0), iota((256, 256), 1)
    return (((i >> 3) == (j & 31)) & ((i & 7) == (j >> 5))).astype(F32).astype(BF16)


def to_expert_rows():
    i, j = iota((256, 256), 0), iota((256, 256), 1)
    place = (((i >> 2) & 3) << 3) | (((i >> 4) & 1) << 2) | (i & 3)
    return (j == ((place << 3) | (i >> 5))).astype(F32).astype(BF16)


def from_expert_rows():
    j, i = iota((256, 256), 0), iota((256, 256), 1)
    place = (((i >> 2) & 3) << 3) | (((i >> 4) & 1) << 2) | (i & 3)
    return (j == ((place << 3) | (i >> 5))).astype(F32).astype(BF16)


def to_expert_cols():
    i, j = iota((256, 256), 0), iota((256, 256), 1)
    spot = (((i >> 2) & 3) << 6) | ((i >> 5) << 3) | ((i & 3) << 1) | ((i >> 4) & 1)
    return (j == spot).astype(F32).astype(BF16)


def expert_order():
    i, j = iota((128, 128), 0), iota((128, 128), 1)
    place = ((i >> 5) << 5) | (((i >> 2) & 3) << 3) | (((i >> 4) & 1) << 2) | (i & 3)
    return (j == place).astype(F32).astype(BF16)


def tile_pair(perm, pieces, put):
    for pair in range(2):
        both = jnp.concatenate(
            [jnp.concatenate(pieces(2 * pair + j), axis=0) for j in range(2)], axis=1
        )
        out = dot(perm, both).astype(BF16)
        for j in range(2):
            put(2 * pair + j, out[:, 128 * j : 128 * (j + 1)])


def row_pair(perm, tiles, put):
    for pair in range(2):
        both = jnp.concatenate([tiles(2 * pair + j) for j in range(2)], axis=1)
        out = dot(perm, both).astype(BF16)
        for j in range(2):
            for b in range(8):
                put(2 * pair + j, b, out[32 * b : 32 * (b + 1), 128 * j : 128 * (j + 1)])


def statistics(moe, grad, gain_ref, stat_ref):
    for b in range(8):
        rows = slice(128 * b, 128 * (b + 1))
        saved = moe[rows, :].astype(F32)
        scaled = gain_ref[...] * grad[rows, :].astype(F32)
        for s, prod in enumerate((saved * saved, saved * scaled)):
            part = (prod[:, :128] + prod[:, 128:]).T
            stat_ref[s, b : b + 1, :] = jnp.sum(part, axis=0, keepdims=True)


def routing(routes_ref, gates_ref, index_ref, stat_ref, spot_ref, gate_ref, pick_ref):
    head = jnp.concatenate(
        [routes_ref[...].astype(F32), gates_ref[...], jnp.zeros((4, 128), F32)], axis=0
    )
    cols = head.T
    lane, row = iota((128, 128), 1), iota((128, 128), 0)
    lane_f = lane.astype(F32)
    below = (lane < row).astype(F32).astype(BF16)
    hot = [(cols[:, k : k + 1] == lane_f).astype(F32) for k in range(2)]
    seen = dot(below, (hot[0] + hot[1]).astype(BF16))
    rank = [jnp.sum(hot[k] * seen, axis=1, keepdims=True) for k in range(2)]
    number = (row + 1).astype(F32)
    index = jnp.zeros((128, 128), F32)
    gate = jnp.zeros((128, 128), F32)
    for k in range(2):
        at = lane_f == rank[k]
        one = hot[k].astype(BF16)
        index += dot(jnp.where(at, number, 0.0).astype(BF16), one, 0, 0)
        gate += dot(one, jnp.where(at, cols[:, 2 + k : 3 + k], 0.0).astype(BF16), 0, 0)
    index_ref[...] = jnp.clip(index[:8].astype(jnp.int32), 0, 128)
    stat_ref[2] = index[:8]
    for z in range(4):
        for x in range(4):
            gate_ref[z, x, :, 0, :] = gate[32 * z + 8 * x : 32 * z + 8 * x + 8, :]
    pick = jnp.zeros((128, 128), F32)
    for k in range(2):
        pick = jnp.where(lane == k, rank[k] * 256.0 + cols[:, k : k + 1], pick)
        pick = jnp.where(lane == 2 + k, cols[:, k : k + 1], pick)
        pick = jnp.where(lane == 4 + k, rank[k], pick)
    pick_ref[...] = pick
    spot_ref[...] = pick.T[:8].astype(jnp.int32)


def token_table(perm, tokens, table_ref):
    for h in range(2):
        table_ref[h, 0] = jnp.zeros((8, 128), BF16)

        def pieces(g, h=h):
            return [
                tokens[32 * g : 32 * (g + 1), 1024 * h + 128 * b : 1024 * h + 128 * (b + 1)]
                for b in range(8)
            ]

        def put(g, tiles, h=h):
            table_ref[h, 1 + 32 * g : 33 + 32 * g] = tiles.reshape(32, 8, 128)

        tile_pair(perm, pieces, put)


def coords():
    ep = lax.axis_index("ep")
    return {"z": ep // 4, "x": ep % 4, "t": lax.axis_index("tp")}


def peers(dim, here):
    if dim != "t":
        return [(here + k) % 4 for k in (2, 1, 3)]
    return [
        (here // 2 + dy) % 4 * 2 + (here % 2 + dc) % 2
        for dy, dc in ((2, 0), (2, 1), (1, 0), (3, 0), (1, 1), (3, 1), (0, 1))
    ]


def others():
    me = coords()
    for dim in "zxt":
        for p in peers(dim, me[dim]):
            place = {**me, dim: p}
            yield dim, p, (place["z"] * 4 + place["x"], place["t"])


def greet():
    for _, _, device in others():
        pl.semaphore_signal(
            pltpu.get_barrier_semaphore(), inc=1, device_id=device, device_id_type=MESH
        )


def cut(ref, axis, index):
    return ref.at[(slice(None),) * axis + (index,)]


class Hop:
    def __init__(self, dim, axis, src, dst, sems, whole=False):
        self.dim, self.axis, self.whole, self.gone = dim, axis, whole, False
        self.src, self.dst, (self.ssem, self.rsem, self.lsem) = src, dst, sems

    def piece(self, index):
        return self.src if self.whole else cut(self.src, self.axis, index)

    def start(self):
        mine = coords()[self.dim]
        for dim, p, device in others():
            if dim == self.dim:
                pltpu.make_async_remote_copy(
                    self.piece(p),
                    cut(self.dst, self.axis, mine),
                    self.ssem,
                    self.rsem,
                    device_id=device,
                    device_id_type=MESH,
                ).start()
        pltpu.make_async_copy(self.piece(mine), cut(self.dst, self.axis, mine), self.lsem).start()

    def remote_part(self):
        return cut(self.dst, self.axis, slice(0, SIZE[self.dim] - 1))

    def arrived(self):
        part = self.remote_part()
        pltpu.make_async_copy(part, part, self.rsem).wait()
        one = cut(self.dst, self.axis, 0)
        pltpu.make_async_copy(one, one, self.lsem).wait()

    def left(self):
        if self.gone:
            return
        self.gone = True
        part = self.remote_part()
        pltpu.make_async_copy(part, part, self.ssem).wait()


class PartHop(Hop):
    def __init__(self, dim, part, src, dst, sems):
        core = lax.axis_index("tp") % 2
        kind = core if part == 0 else 1 - core
        self.cross = dim == "t" and part == 1
        self.far = dst.at[:, :, :, 1 - kind]
        src, dst = src.at[:, :, :, kind], dst.at[:, :, :, kind]
        super().__init__(dim, AXIS[dim], src, dst, sems)

    def start(self):
        if self.dim != "t":
            super().start()
            return
        me = coords()
        mine, core = me["t"] // 2, me["t"] % 2
        for k in (2, 1, 3, 0) if self.cross else (2, 1, 3):
            p = (mine + k) % 4
            place = 2 * p + (1 - core if self.cross else core)
            pltpu.make_async_remote_copy(
                cut(self.src, 2, p),
                cut(self.far if self.cross else self.dst, 2, mine),
                self.ssem,
                self.rsem,
                device_id=(me["z"] * 4 + me["x"], place),
                device_id_type=MESH,
            ).start()
        if not self.cross:
            pltpu.make_async_copy(cut(self.src, 2, mine), cut(self.dst, 2, mine), self.lsem).start()

    def remote_part(self):
        return self.dst if self.cross else cut(self.dst, self.axis, slice(0, 3))

    def arrived(self):
        if self.cross:
            pltpu.make_async_copy(self.dst, self.dst, self.rsem).wait()
        else:
            super().arrived()


def pack(index_ref, rank, table_ref, half, dst):
    def body(i, carry):
        for t in range(8):
            dst[i // 4, i % 4, t] = table_ref[half, index_ref[rank, i * 8 + t]]
        return carry

    lax.fori_loop(0, 16, body, 0)


def mega_kernel(
    routes_any, gates_any, gain_any, tokens_any, moe_any, grad_any, wg_any, wu_any, wd_any,
    back_ref, slope_ref, spot_ref, pick_ref, gate_grad, up_grad, down_grad,
    routes_ref, gates_ref, gain_ref, tokens, moe, grad, index_v, index_ref, gate_src, table_ref, stat_ref,
    wg_t, wu_t, wd_t, t_src, t_one, t_two, t_out, c_src, c_one, c_two, c_out, r_src, r_one, r_two,
    g_one, g_two, g_out, q_src, q_one, q_two, s_in, cot_parts, index_cols, gate_cols,
    x_rows, x_t, d_gate, d_up, hidden, pre_gate, pre_up, cot_rows, back_rows, slope,
    ssem, rsem, lsem, misc, wsem,
):
    wg, wu = gate_grad, up_grad
    loads = [
        pltpu.make_async_copy(a, b, wsem.at[i])
        for i, (a, b) in enumerate(
            (
                (moe_any, moe), (grad_any, grad), (tokens_any, tokens),
                (wg_any, gate_grad), (wu_any, up_grad), (wd_any, down_grad),
                (routes_any, routes_ref), (gates_any, gates_ref), (gain_any, gain_ref),
            )
        )
    ]
    loaded = set()

    def need(*which):
        for i in which:
            if i not in loaded:
                loads[i].wait()
                loaded.add(i)

    greet()
    for i in (6, 7, 8, 0, 1, 2, 3, 4, 5):
        loads[i].start()
    slope[...] = jnp.zeros((128, 128), F32)
    need(6, 7, 8)
    routing(routes_ref, gates_ref, index_v, stat_ref, spot_ref, gate_src, pick_ref)
    index_copy = pltpu.make_async_copy(index_v, index_ref, wsem.at[9])
    index_copy.start()
    need(0, 1)
    statistics(moe, grad, gain_ref, stat_ref)
    need(2)
    token_table(to_tiles(), tokens, table_ref)
    index_copy.wait()
    families = {
        "T": (t_src, t_one, t_two, t_out),
        "C": (c_src, c_one, c_two, c_out),
        "R": (r_src, r_one, r_two, back_ref),
    }
    hops = {}
    every = []

    def small(i):
        return tuple(misc.at[i, j] for j in range(3))

    stat_hop = Hop("t", 0, stat_ref, s_in, small(0), whole=True)
    gate_hops = [
        Hop(d, AXIS[d], a, b, small(2 + i))
        for i, (d, a, b) in enumerate(
            (("x", gate_src, g_one), ("t", g_one, g_two), ("z", g_two, g_out))
        )
    ]
    slope_hops = [
        Hop(d, AXIS[d], a, b, small(5 + i))
        for i, (d, a, b) in enumerate(
            (("x", q_src, q_one), ("t", q_one, q_two), ("z", q_two, slope_ref))
        )
    ]

    def begin(hop):
        hop.start()
        every.append(hop)

    def norm_statistics():
        begin(stat_hop)
        begin(gate_hops[0])

    def cotangents():
        stat_hop.arrived()
        total = s_in[0]
        for p in range(1, 8):
            total += s_in[p]
        inv = lax.rsqrt(total[0] / 2048.0 + epsilon)
        cols = jnp.concatenate([inv, inv**3 * total[1] / 2048.0], axis=0).T

        for b in range(8):
            rows = slice(128 * b, 128 * (b + 1))
            scaled = gain_ref[...] * grad[rows, :].astype(F32)
            saved = moe[rows, :].astype(F32)
            cot_parts[b] = (
                cols[:, b : b + 1] * scaled - saved * cols[:, 8 + b : 9 + b]
            ).astype(BF16)
        index_cols[...] = jnp.concatenate(
            [s_in[b, 2] for b in range(8)] + [jnp.zeros((64, 128), F32)], axis=0
        ).T
        gate_hops[0].arrived()
        begin(gate_hops[1])

    def pack_cotangents(c, dst):
        rank, half = c // 2, c % 2
        number = (iota((128, 128), 1) + 1).astype(F32)
        parts = []
        for b in range(4 * half, 4 * half + 4):
            index = index_cols[:, 8 * b + rank : 8 * b + rank + 1]
            chosen = (index == number).astype(F32).astype(BF16)
            parts.append(dot(chosen, cot_parts[b]).astype(BF16))

        def pieces(g):
            return [
                part[32 * g : 32 * (g + 1), 128 * b : 128 * (b + 1)]
                for part in parts
                for b in range(2)
            ]

        def put(g, tiles):
            dst[g] = tiles.reshape(4, 8, 8, 128)

        tile_pair(to_tiles(), pieces, put)

    def unpack(src, dst, row, half):
        def put(g, b, rows):
            dst[
                row + 32 * g : row + 32 * (g + 1), 1024 * half + 128 * b : 1024 * half + 128 * b + 128
            ] = rows

        row_pair(to_expert_rows(), lambda g: src[g].reshape(256, 128), put)

    def unpack_cotangents(src, row, half):
        perm = to_expert_cols()
        for pair in range(2):
            both = jnp.concatenate([src[2 * pair + j].reshape(256, 128) for j in range(2)], axis=1)
            out = dot(perm, both).astype(BF16)
            for j in range(2):
                at = row + 32 * (2 * pair + j) + 16 * half
                for b in range(16):
                    cot_rows[at : at + 16, 128 * b : 128 * (b + 1)] = out[
                        16 * b : 16 * (b + 1), 128 * j : 128 * (j + 1)
                    ]

    def hidden_inputs(r):
        need(3, 4)
        for h in range(2):
            hops["T", 2 * r + h][2].arrived()
            unpack(t_out.at[2 * r + h], x_rows, 0, h)

        def body(n, carry):
            cols = pl.ds(pl.multiple_of(n * 256, 256), 256)
            x = x_rows[...]
            pre_gate[r, :, cols] = dot(x, wg[:, cols])
            pre_up[r, :, cols] = dot(x, wu[:, cols])
            return carry

        lax.fori_loop(0, 3, body, 0)

        def turned(n, carry):
            cols = pl.ds(pl.multiple_of(n * 256, 256), 256)
            x_t[cols, 128 * r : 128 * (r + 1)] = x_rows[:, cols].T
            return carry

        lax.fori_loop(0, 8, turned, 0)

    def half_back(r, h):
        rows = slice(128 * r, 128 * (r + 1))

        def body(n, carry):
            wide = pl.ds(pl.multiple_of(1024 * h + n * 512, 512), 512)
            total = dot(d_gate[rows, :], wg_t[:, wide]) + dot(d_up[rows, :], wu_t[:, wide])
            back_rows[:, pl.ds(pl.multiple_of(n * 512, 512), 512)] = total.astype(BF16)
            return carry

        lax.fori_loop(0, 2, body, 0)

        def pieces(g):
            return [
                back_rows[32 * g : 32 * (g + 1), 128 * b : 128 * (b + 1)] for b in range(8)
            ]

        def put(g, tiles):
            r_src[2 * r + h, g] = tiles.reshape(4, 4, 2, 8, 128)

        tile_pair(from_expert_rows(), pieces, put)

    def gate_of(r):
        return gate_cols[:, r : r + 1]

    def slopes(r):
        if r == 2:
            gate_hops[2].arrived()
            gates = jnp.concatenate(
                [g_out[z, x][:, 0, :] for z in range(4) for x in range(4)], axis=0
            )
            gate_cols[...] = dot(expert_order(), gates.astype(BF16))
        for h in range(2):
            hops["C", 2 * r + h][2].arrived()
            unpack_cotangents(c_out.at[2 * r + h], 128 * r, h)
        gate = gate_of(r)
        rows = slice(128 * r, 128 * (r + 1))

        def body(n, carry):
            cols = pl.ds(pl.multiple_of(n * 256, 256), 256)
            hid_grad = dot(cot_rows[rows, :], wd_t[:, cols])
            p_gate, p_up = pre_gate[r, :, cols], pre_up[r, :, cols]
            sig = jax.nn.sigmoid(p_gate)
            act = p_gate * sig
            hid = act * p_up
            d_hid = gate * hid_grad
            d_gate[rows, cols] = (d_hid * p_up * sig * (1.0 + p_gate * (1.0 - sig))).astype(BF16)
            d_up[rows, cols] = (d_hid * act).astype(BF16)
            hidden[rows, cols] = hid.astype(BF16)
            return carry + jnp.sum(hid * hid_grad, axis=1, keepdims=True)

        total = lax.fori_loop(0, 3, body, jnp.zeros((128, 1), F32))
        slope[...] = jnp.where(iota((128, 128), 1) == r, total, slope[...])
        half_back(r, 0)

    def rest(r):
        half_back(r, 1)
        if r == 1:
            slope[...] = dot(expert_order(), slope[...].astype(BF16), 0, 0)
            for z in range(4):
                for x in range(4):
                    q_src[z, x, :, 0, :] = slope[32 * z + 8 * x : 32 * z + 8 * x + 8, :]
            begin(slope_hops[0])

    def turn(src, dst):
        def body(n, carry):
            rows = pl.ds(pl.multiple_of(n * 256, 256), 256)
            dst[:, rows] = src[rows, :].T
            return carry

        lax.fori_loop(0, src.shape[0] // 256, body, 0)

    def turn_weight(i):
        if i == 0:
            need(5)
            turn(down_grad, wd_t)
        elif i == 1:
            need(3)
            turn(gate_grad, wg_t)
        else:
            need(4)
            turn(up_grad, wu_t)

    def scale(r):
        rows = slice(128 * r, 128 * (r + 1))
        cot_rows[rows, :] = (gate_of(r) * cot_rows[rows, :].astype(F32)).astype(BF16)

    def weight_grad(i):
        if i >= 8:
            rows = slice(256 * (i - 8), 256 * (i - 7))
            down_grad[rows, :] = dot(hidden[:, rows], cot_rows[...], 0, 0).astype(BF16)
            return
        out, right = ((gate_grad, d_gate), (up_grad, d_up))[i // 4]

        def body(n, carry):
            rows = pl.ds(pl.multiple_of(512 * (i % 4) + n * 256, 256), 256)
            out[rows, :] = dot(x_t[rows, :], right[...]).astype(BF16)
            return carry

        lax.fori_loop(0, 2, body, 0)

    early = [step for step in PLAN if step[0] == "T"][:3]
    for step in early:
        c = int(step[1])
        pack(index_ref, c // 2, table_ref, c % 2, t_src.at[c])
    lasts = (103, 115)
    for i, step in enumerate(PLAN):
        kind = step[0]
        if step == "bar":
            pl.semaphore_wait(pltpu.get_barrier_semaphore(), 13)
        elif step == "stat":
            norm_statistics()
        elif step == "cot":
            cotangents()
        elif kind == "A":
            hidden_inputs(int(step[1]))
        elif kind == "B":
            slopes(int(step[1]))
        elif kind == "D":
            rest(int(step[1]))
        elif kind == "M":
            turn_weight(int(step[1]))
        elif kind == "S":
            scale(int(step[1]))
        elif kind == "W":
            weight_grad(int(step[1:]))
        else:
            c, d = int(step[1]), step[2]
            part = step[3:]
            done = hops.setdefault((kind, c, part) if part else (kind, c), [])
            k = len(done)
            bufs = families[kind]
            if k:
                done[-1].arrived()
            elif kind == "T" and step not in early:
                pack(index_ref, c // 2, table_ref, c % 2, t_src.at[c])
            elif kind == "C":
                pack_cotangents(c, c_src.at[c])
            if part:
                n = 16 + 2 * c + int(part)
                hop = PartHop(
                    d, int(part), bufs[k].at[c], bufs[k + 1].at[c],
                    (ssem.at[n, k], rsem.at[n, k], lsem.at[n, k]),
                )
            else:
                n = "TC".index(kind) * 8 + c
                hop = Hop(
                    d, AXIS[d], bufs[k].at[c], bufs[k + 1].at[c],
                    (ssem.at[n, k], rsem.at[n, k], lsem.at[n, k]),
                )
            begin(hop)
            done.append(hop)
            if i == 22:
                gate_hops[1].arrived()
                begin(gate_hops[2])
            if i in (lasts[0], lasts[1]):
                slope_hops[lasts.index(i)].arrived()
                begin(slope_hops[lasts.index(i) + 1])
    for c in range(8):
        hops["R", c, "0"][2].arrived()
        hops["R", c, "1"][2].arrived()
    slope_hops[2].arrived()
    for hop in every:
        hop.left()


def finish_kernel(
    spot_any, back_ref, slope_ref, pick_ref, gate_grad, up_grad, down_grad,
    token_out, gates_out, gate_out, up_out, down_out, spot_ref, token_ref, gates_ref, sums, sem,
):
    copies = []
    for i, (a, b) in enumerate(((gate_grad, gate_out), (up_grad, up_out), (down_grad, down_out))):
        size = a.shape[0] // 4
        for j in range(4):
            part = pl.ds(j * size, size)
            copies.append(pltpu.make_async_copy(a.at[part], b.at[0, part], sem.at[4 * i + j]))
    spots = pltpu.make_async_copy(spot_any, spot_ref, sem.at[12])
    spots.start()
    for copy in copies:
        copy.start()
    spots.wait()

    def body(i, carry):
        for j in range(16):
            t = i * 16 + j
            for h in range(2):
                one = back_ref[spot_ref[0, t] + 128 * h].astype(F32)
                two = back_ref[spot_ref[1, t] + 128 * h].astype(F32)
                sums[h, t] = (one + two).astype(BF16)
        return carry

    lax.fori_loop(0, 8, body, 0)
    perm = to_rows()
    for h in range(2):

        def put(g, b, rows, h=h):
            token_ref[32 * g : 32 * (g + 1), 1024 * h + 128 * b : 1024 * h + 128 * (b + 1)] = rows

        row_pair(perm, lambda g, h=h: sums[h, 32 * g : 32 * (g + 1)].reshape(256, 128), put)
    copies.append(pltpu.make_async_copy(token_ref, token_out, sem.at[13]))
    copies[-1].start()
    slope = slope_ref[:, 0, :].astype(BF16)
    pick = pick_ref[...]
    lane = iota((128, 128), 1)
    lane_f = lane.astype(F32)
    both = jnp.zeros((128, 128), F32)
    for k in range(2):
        one = (pick[:, 2 + k : 3 + k] == lane_f).astype(F32).astype(BF16)
        mine = jnp.where(lane_f == pick[:, 4 + k : 5 + k], dot(one, slope), 0.0)
        both = jnp.where(lane == k, jnp.sum(mine, axis=1, keepdims=True), both)
    gates_ref[...] = both.T[:2].astype(BF16)
    copies.append(pltpu.make_async_copy(gates_ref, gates_out, sem.at[14]))
    copies[-1].start()
    for copy in copies:
        copy.wait()


def struct(shape, dtype=BF16):
    return jax.ShapeDtypeStruct(shape, dtype)


def local(tokens, routes, gates, w_gate, w_up, w_down, moe_out, norm_gain, out_grad):
    pieces = (8, 4, 4, 8, 8, 128)
    halves = (8, 4, 4, 4, 2, 8, 128)
    lanes = (4, 4, 8, 1, 128)
    deep, flat = (2048, 768), (768, 2048)
    rows, inner = (512, 2048), (512, 768)
    back, slope, spot, pick, gate_grad, up_grad, down_grad = pl.pallas_call(
        mega_kernel,
        out_shape=(
            pltpu.VMEM(halves, BF16),
            pltpu.VMEM(lanes, F32),
            pltpu.VMEM((8, 128), jnp.int32),
            pltpu.VMEM((128, 128), F32),
            pltpu.VMEM(deep, BF16),
            pltpu.VMEM(deep, BF16),
            pltpu.VMEM(flat, BF16),
        ),
        in_specs=[ANY] * 9,
        out_specs=(VMEM,) * 7,
        scratch_shapes=[
            pltpu.VMEM((2, 128), jnp.int32),
            pltpu.VMEM((2, 128), F32),
            pltpu.VMEM((1, 256), F32),
            pltpu.VMEM((128, 2048), BF16),
            pltpu.VMEM((1024, 256), BF16),
            pltpu.VMEM((1024, 256), BF16),
            pltpu.VMEM((8, 128), jnp.int32),
            pltpu.SMEM((8, 128), jnp.int32),
            pltpu.VMEM(lanes, F32),
            pltpu.VMEM((2, 129, 8, 128), BF16),
            pltpu.VMEM((3, 8, 128), F32),
            pltpu.VMEM(flat, BF16),
            pltpu.VMEM(flat, BF16),
            pltpu.VMEM(deep, BF16),
            *[pltpu.VMEM(pieces, BF16)] * 8,
            *[pltpu.VMEM(halves, BF16)] * 3,
            *[pltpu.VMEM(lanes, F32)] * 6,
            pltpu.VMEM((8, 3, 8, 128), F32),
            pltpu.VMEM((8, 128, 256), BF16),
            pltpu.VMEM((128, 128), F32),
            pltpu.VMEM((128, 128), F32),
            pltpu.VMEM((128, 2048), BF16),
            pltpu.VMEM((2048, 512), BF16),
            pltpu.VMEM(inner, BF16),
            pltpu.VMEM(inner, BF16),
            pltpu.VMEM(inner, BF16),
            pltpu.VMEM((4, 128, 768), F32),
            pltpu.VMEM((4, 128, 768), F32),
            pltpu.VMEM(rows, BF16),
            pltpu.VMEM((128, 1024), BF16),
            pltpu.VMEM((128, 128), F32),
            pltpu.SemaphoreType.DMA((32, 3)),
            pltpu.SemaphoreType.DMA((32, 3)),
            pltpu.SemaphoreType.DMA((32, 3)),
            pltpu.SemaphoreType.DMA((8, 3)),
            pltpu.SemaphoreType.DMA((10,)),
        ],
        compiler_params=pltpu.CompilerParams(
            collective_id=0, has_side_effects=True, vmem_limit_bytes=48 << 20
        ),
        name="exchange",
    )(
        routes.T, gates.T, norm_gain.reshape(1, 256), tokens, moe_out, out_grad,
        w_gate[0], w_up[0], w_down[0],
    )
    token_grad, gates_grad, *grads = pl.pallas_call(
        finish_kernel,
        out_shape=(
            struct((128, 2048)),
            struct((2, 128)),
            struct((1, *deep)),
            struct((1, *deep)),
            struct((1, *flat)),
        ),
        in_specs=[VMEM] * 7,
        out_specs=(ANY,) * 5,
        scratch_shapes=[
            pltpu.SMEM((8, 128), jnp.int32),
            pltpu.VMEM((128, 2048), BF16),
            pltpu.VMEM((2, 128), BF16),
            pltpu.VMEM((2, 128, 8, 128), BF16),
            pltpu.SemaphoreType.DMA((15,)),
        ],
        compiler_params=pltpu.CompilerParams(vmem_limit_bytes=8 << 20),
        name="finish",
    )(spot, back.reshape(1024, 8, 128), slope.reshape(128, 1, 128), pick, gate_grad, up_grad, down_grad)
    return (token_grad, gates_grad.T, *grads)


def solution(mesh):
    split = P(("ep", "tp"), None)
    expert = P(("ep", "tp"), None, None)
    in_specs = (split, split, split, expert, expert, expert, P("ep", "tp"), P("tp"), P("ep", "tp"))
    out_specs = (split, split, expert, expert, expert)
    return jax.shard_map(local, mesh=mesh, in_specs=in_specs, out_specs=out_specs, check_vma=False)
```
